256 devices in a mesh: sp: 32 (over z, x), fs: 4 (over y), tp: 2 (over core).
Axes of the slice: x: 4, y: 4, z: 8, core: 2. Of those that a mesh axis runs over, the one named last changes fastest.
Arguments:
- inputs: bfloat16 [4, 8192, 2048], P('fs', ('sp', 'tp')), may hold values from -6 to 6
- norm_gain: float32 [2048], replicated, may hold values from 0.1 to 1.9
- w_glu_value: bfloat16 [2048, 1024], P(None, 'tp'), may hold values from -0.125 to 0.125
- w_glu_gate: bfloat16 [2048, 1024], P(None, 'tp'), may hold values from -0.125 to 0.125
- w_query_one: bfloat16 [2048, 512], P(None, 'tp'), may hold values from -2.5 to 2.5
- w_query_two: bfloat16 [2048, 512], P(None, 'tp'), may hold values from -2.5 to 2.5
- w_key_one: bfloat16 [2048, 512], P(None, 'tp'), may hold values from -2.5 to 2.5
- w_key_two: bfloat16 [2048, 512], P(None, 'tp'), may hold values from -2.5 to 2.5
- w_value: bfloat16 [2048, 1024], P(None, 'tp'), may hold values from -0.125 to 0.125
- conv_kernel: bfloat16 [31, 1024], P(None, 'tp'), may hold values from -1 to 1
- conv_gain: float32 [1024], P('tp'), may hold values from 0.1 to 1.9
- head_gain: float32 [128], replicated, may hold values from 0.1 to 1.9
- lambda_head: float32 [8], P('tp'), may hold values from 0.3 to 0.8
- w_out_conv: bfloat16 [1024, 2048], P('tp', 'fs'), may hold values from -0.125 to 0.125
- w_out_attn: bfloat16 [1024, 2048], P('tp', 'fs'), may hold values from -0.125 to 0.125
Outputs:
- mixed: bfloat16 [4, 8192, 2048], P('fs', ('sp', 'tp'))
- log_sums: float32 [4, 2, 8, 8192], P('fs', None, 'tp', 'sp')
The draws below stay inside these ranges and needn't reach their ends.
All inputs are finite; a program needn't handle non-finite values.
Results may differ from the reference program's by a relative error of at most 0.013.
Values may be sent and summed in bfloat16 or wider, within the bound.
A program may use at most 128 MiB of HBM per device.

```python
import jax
import jax.numpy as jnp
from jax import lax

D = 2048
DC = 1024
H = 8
KVH = 8
HD = 64
VD = 128
CW = 31
SEG = 64
SEQ = 8192
BATCH = 4
DA = 1024


def query_key_pair(key, which):
    base_key = jax.random.fold_in(key, 7 + which)
    spread = (3.0 / D) ** 0.5
    key_weight = jax.random.normal(jax.random.fold_in(base_key, 1), (D, KVH * HD), jnp.float32) * spread
    query_weight = jax.random.normal(jax.random.fold_in(base_key, 2), (D, H * HD), jnp.float32) * spread
    return (jnp.clip(query_weight, -2.5, 2.5), jnp.clip(key_weight, -2.5, 2.5))


def draw_w_query_one(key, part):
    return query_key_pair(key, 1)[0].astype(jnp.bfloat16)


def draw_w_key_one(key, part):
    return query_key_pair(key, 1)[1].astype(jnp.bfloat16)


def draw_w_query_two(key, part):
    return query_key_pair(key, 2)[0].astype(jnp.bfloat16)


def draw_w_key_two(key, part):
    return query_key_pair(key, 2)[1].astype(jnp.bfloat16)


def steps_of(key, extent, pieces, low, high):
    gain, own = 1.0, jax.random.fold_in(key, 6)
    for dim, parts in pieces:
        heights = jnp.exp(jax.random.uniform(jax.random.fold_in(own, dim), (parts,), jnp.float32, low / len(pieces), high / len(pieces)))
        gain = gain * jnp.repeat(heights, extent[dim] // parts).reshape([-1 if axis == dim else 1 for axis in range(len(extent))])
    return gain


def gaussian(stream_key, shape, scale, most, cuts=(), held_as=jnp.bfloat16):
    loudness = steps_of(stream_key, shape, cuts, -0.22, 0.18) if cuts else 1.0
    result = jax.random.normal(stream_key, shape, jnp.float32) * scale * loudness
    return jnp.minimum(jnp.maximum(result, -most), most).astype(held_as)


def setup_inputs(seed: int = 0) -> dict:
    streams_of = jax.random.split(jax.random.key(seed), 16)
    inputs = gaussian(streams_of[0], (BATCH, SEQ, D), 1.0, 6.0, ((0, 4), (1, 64)))
    norm_gain = jnp.clip(1.0 + 0.18 * jax.random.normal(streams_of[1], (D,), jnp.float32), 0.1, 1.9)
    w_glu_value = gaussian(streams_of[2], (D, DC), D ** -0.5, 0.125, ((1, 2),))
    w_glu_gate = gaussian(streams_of[3], (D, DC), D ** -0.5, 0.125, ((1, 2),))
    w_query_one = draw_w_query_one(jax.random.fold_in(streams_of[15], 71), 0)
    w_query_two = draw_w_query_two(jax.random.fold_in(streams_of[15], 71), 0)
    w_key_one = draw_w_key_one(jax.random.fold_in(streams_of[15], 71), 0)
    w_key_two = draw_w_key_two(jax.random.fold_in(streams_of[15], 71), 0)
    w_value = gaussian(streams_of[8], (D, KVH * VD), D ** -0.5, 0.125, ((1, 2),))
    conv_kernel = gaussian(streams_of[9], (CW, DC), CW ** -0.5, 1.0, ((1, 2),))
    conv_gain = jnp.clip(1.0 + 0.18 * jax.random.normal(streams_of[10], (DC,), jnp.float32), 0.1, 1.9)
    head_gain = jnp.clip(1.0 + 0.18 * jax.random.normal(streams_of[11], (VD,), jnp.float32), 0.1, 1.9)
    lambda_head = jnp.clip(0.3 + 0.5 * jax.random.uniform(streams_of[12], (H,), jnp.float32) ** steps_of(streams_of[12], (H,), ((0, 2),), -0.2, 0.2), 0.3, 0.8)
    w_out_conv = gaussian(streams_of[13], (DC, D), (DC + DA) ** -0.5, 0.125, ((0, 2), (1, 4)))
    w_out_attn = gaussian(streams_of[14], (DA, D), (DC + DA) ** -0.5, 0.125, ((0, 2), (1, 4)))
    return dict(inputs=inputs, norm_gain=norm_gain, w_glu_value=w_glu_value, w_glu_gate=w_glu_gate, w_query_one=w_query_one, w_query_two=w_query_two, w_key_one=w_key_one, w_key_two=w_key_two, w_value=w_value, conv_kernel=conv_kernel, conv_gain=conv_gain, head_gain=head_gain, lambda_head=lambda_head, w_out_conv=w_out_conv, w_out_attn=w_out_attn)


NEG_FILL = -1e+30
EPSILON = 1e-05
HEAD_SCALE = 0.8

def one_sequence(seq_rows, norm_gain, w_glu_value, w_glu_gate, w_query_one, w_query_two, w_key_one, w_key_two, w_value, conv_kernel, conv_gain, head_gain, lambda_head, w_out_conv, w_out_attn):
    rows_f = seq_rows.astype(jnp.float32)
    normed = (rows_f * lax.rsqrt(lax.optimization_barrier(jnp.mean(rows_f * rows_f, axis=-1, keepdims=True)) + EPSILON) * norm_gain).astype(jnp.bfloat16)

    def project(weight):
        return jnp.dot(normed, weight, preferred_element_type=jnp.float32).astype(jnp.bfloat16)
    glu_value = project(w_glu_value)
    glu_gate = project(w_glu_gate)
    query_one = project(w_query_one)
    query_two = project(w_query_two)
    key_one = project(w_key_one)
    key_two = project(w_key_two)
    values = project(w_value)
    gated = (glu_value.astype(jnp.float32) * jax.nn.sigmoid(glu_gate.astype(jnp.float32))).astype(jnp.bfloat16)
    extended = jnp.concatenate([jnp.zeros((CW - 1, DC), jnp.bfloat16), gated], axis=0).astype(jnp.float32)
    kernel_f = conv_kernel.astype(jnp.float32)
    convolved = jnp.zeros((SEQ, DC), jnp.float32)
    for tap_index in range(CW):
        convolved = convolved + kernel_f[tap_index][None, :] * extended[tap_index:tap_index + SEQ]
    row_mean = lax.optimization_barrier(jnp.mean(convolved, axis=-1, keepdims=True))
    row_square = lax.optimization_barrier(jnp.mean(convolved * convolved, axis=-1, keepdims=True))
    conv_out = jax.nn.silu((convolved - row_mean) * lax.rsqrt(row_square - row_mean * row_mean + EPSILON) * conv_gain).astype(jnp.bfloat16)
    group = H // KVH
    query_one_r = query_one.reshape(SEQ, KVH, group, HD).astype(jnp.float32)
    query_two_r = query_two.reshape(SEQ, KVH, group, HD).astype(jnp.float32)
    key_one_r = key_one.reshape(SEQ, KVH, HD).astype(jnp.float32)
    key_two_r = key_two.reshape(SEQ, KVH, HD).astype(jnp.float32)
    values_r = values.reshape(SEQ, KVH, VD).astype(jnp.float32)
    lambda_r = lambda_head.reshape(KVH, group)
    score_scale = HD ** (-0.5)
    block_rows = min(512, SEQ)
    attn_blocks = []
    log_blocks = []
    for block_start in range(0, SEQ, block_rows):
        block_end = min(block_start + block_rows, SEQ)
        query_pos = jnp.arange(block_start, block_end, dtype=jnp.int32)
        key_pos = jnp.arange(0, block_end, dtype=jnp.int32)
        allowed = ((key_pos // SEG)[None, :] <= (query_pos // SEG)[:, None])[:, None, None, :]
        pooled_list = []
        log_list = []
        for queries, key_rows in ((query_one_r, key_one_r), (query_two_r, key_two_r)):
            scores = jnp.einsum('tgrd,kgd->tgrk', queries[block_start:block_end], key_rows[:block_end]) * score_scale
            scores = jnp.where(allowed, scores, NEG_FILL)
            row_max = lax.optimization_barrier(jnp.max(scores, axis=-1))
            weights = jnp.where(allowed, jnp.exp(scores - row_max[..., None]), 0.0)
            weight_sum = lax.optimization_barrier(jnp.sum(weights, axis=-1))
            log_list.append(row_max + jnp.log(weight_sum))
            pooled = jnp.einsum('tgrk,kgv->tgrv', weights.astype(jnp.bfloat16).astype(jnp.float32), values_r[:block_end])
            pooled_list.append(pooled / weight_sum[..., None])
        head_out = pooled_list[0] - lambda_r[None, :, :, None] * pooled_list[1]
        head_out = head_out * lax.rsqrt(lax.optimization_barrier(jnp.mean(head_out * head_out, axis=-1, keepdims=True)) + EPSILON) * head_gain * HEAD_SCALE
        attn_blocks.append(head_out.astype(jnp.bfloat16).reshape(block_end - block_start, H * VD))
        log_blocks.append(jnp.stack(log_list, axis=0).reshape(2, block_end - block_start, H))
    attn_out = jnp.concatenate(attn_blocks, axis=0)
    log_sums = jnp.transpose(jnp.concatenate(log_blocks, axis=1), (0, 2, 1))
    mixed = jnp.dot(conv_out, w_out_conv, preferred_element_type=jnp.float32) + jnp.dot(attn_out, w_out_attn, preferred_element_type=jnp.float32)
    return (mixed.astype(jnp.bfloat16), log_sums)

def reference(inputs, norm_gain, w_glu_value, w_glu_gate, w_query_one, w_query_two, w_key_one, w_key_two, w_value, conv_kernel, conv_gain, head_gain, lambda_head, w_out_conv, w_out_attn):

    def per_sequence(seq_rows):
        return one_sequence(seq_rows, norm_gain, w_glu_value, w_glu_gate, w_query_one, w_query_two, w_key_one, w_key_two, w_value, conv_kernel, conv_gain, head_gain, lambda_head, w_out_conv, w_out_attn)
    mixed, log_sums = lax.map(per_sequence, inputs)
    return (mixed, log_sums)
```

```python
import jax
import jax.numpy as jnp
from jax import lax
from jax.experimental import pallas as pl
from jax.experimental.pallas import tpu as pltpu
from jax.sharding import PartitionSpec as P

D = 2048
DC = 1024
HD = 64
CW = 31
NZ = 8
NX = 4
NY = 4
HALF = 128
NEG_FILL = -1e30
EPSILON = 1e-05
HEAD_SCALE = 0.8
MESH = pl.DeviceIdType.MESH
F32 = jnp.float32
BF16 = jnp.bfloat16
Z_ORDER = (0, 1, 7, 2, 6, 3, 5, 4)


def remote(src, dst, send_sem, recv_sem, device):
    return pltpu.make_async_remote_copy(
        src_ref=src,
        dst_ref=dst,
        send_sem=send_sem,
        recv_sem=recv_sem,
        device_id=device,
        device_id_type=MESH,
    )


def kernel(
    x_ref,
    gain_ref,
    ck_ref,
    cg_ref,
    hg_ref,
    lam_ref,
    wgv_hbm,
    wgg_hbm,
    wq1_hbm,
    wq2_hbm,
    wk1_hbm,
    wk2_hbm,
    wv_hbm,
    woc_hbm,
    woa_hbm,
    out_ref,
    log_ref,
    wgv,
    wgg,
    wq1,
    wq2,
    wk1,
    wk2,
    wv,
    normed,
    kv_send,
    q_send,
    kv_buf,
    q_raw,
    qs,
    gated_ext,
    halo_send,
    halo_recv,
    convd,
    sums_send,
    sums_recv,
    conv_full,
    conv_send,
    m_buf,
    acc,
    ret_send,
    attn_buf,
    lsend,
    log_buf,
    lam_recv,
    w_buf,
    acc_out,
    load_sem,
    norm_sem,
    kv_ss,
    q_ss,
    kv_rs,
    q_rs,
    xs_ss,
    xs_rs,
    d_ss,
    d_rs,
    halo_sem,
    sums_sem,
    cx_sem,
    lam_sem,
    ret_ss,
    ret_rs,
    log_ss,
    log_rs,
    w_ss,
    w_rs,
    wd_ss,
    wd_rs,
    own_sem,
):
    me = lax.axis_index("sp")
    y = lax.axis_index("fs")
    c = lax.axis_index("tp")
    z, x = me // NX, me % NX
    other = 1 - c
    xr, xl, xo = (x + 1) % NX, (x + 3) % NX, (x + 2) % NX
    yr, yl, yo = (y + 1) % NY, (y + 3) % NY, (y + 2) % NY
    src_tp = z // 4
    partner = {"tp": other}
    right = {"sp": z * NX + xr}
    left = {"sp": z * NX + xl}
    up = {"fs": yr}
    down = {"fs": yl}
    following = {"sp": (me + 1) % (NZ * NX)}
    preceding = {"sp": (me + NZ * NX - 1) % (NZ * NX)}
    pending = []

    loads = []
    for index, (src, dst) in enumerate(
        ((wv_hbm, wv), (wk1_hbm, wk1), (wk2_hbm, wk2), (wq1_hbm, wq1), (wq2_hbm, wq2),
         (wgv_hbm, wgv), (wgg_hbm, wgg))
    ):
        loads.append(pltpu.make_async_copy(src, dst, load_sem.at[index]))
        loads[-1].start()

    barrier = pltpu.get_barrier_semaphore()
    for device in (partner, right, left, up, down, following, preceding):
        pl.semaphore_signal(barrier, inc=1, device_id=device, device_id_type=MESH)
    for step in range(1, NZ):
        for core in range(2):
            pl.semaphore_signal(
                barrier,
                inc=1,
                device_id={"sp": ((z + step) % NZ) * NX + x, "tp": core},
                device_id_type=MESH,
            )

    my_rows = pl.multiple_of(c * HALF, HALF)
    for part in range(4):
        rows_f = x_ref[part * 32 : part * 32 + 32, :].astype(F32)
        scale = lax.rsqrt(jnp.mean(rows_f * rows_f, axis=-1, keepdims=True) + EPSILON)
        normed[pl.ds(my_rows + part * 32, 32), :] = (rows_f * scale * gain_ref[...]).astype(BF16)

    pl.semaphore_wait(barrier, 7 + 2 * (NZ - 1))

    mine = normed.at[pl.ds(my_rows, HALF), :]
    norm_copy = remote(mine, mine, norm_sem.at[0], norm_sem.at[1], partner)
    norm_copy.start()
    lam_copy = remote(lam_ref, lam_recv, lam_sem.at[0], lam_sem.at[1], partner)
    lam_copy.start()
    pending.append(lam_copy)

    w_hbm = (woc_hbm, woa_hbm)
    own_w = []
    for kind in range(2):
        own = pltpu.make_async_copy(w_hbm[kind], w_buf.at[y, c, kind], own_sem.at[kind])
        own.start()
        own_w.append(own)
    for kind in (0, 1):
        copy = remote(w_hbm[kind], w_buf.at[y, c, kind], w_ss.at[0, kind], w_rs.at[0, kind], up)
        copy.start()
        pending.append(copy)
        copy = remote(
            w_hbm[1 - kind], w_buf.at[y, c, 1 - kind], w_ss.at[1, 1 - kind], w_rs.at[1, 1 - kind], down
        )
        copy.start()
        pending.append(copy)

    norm_copy.wait()

    def project(load, weight):
        load.wait()
        return jnp.dot(normed[...], weight[...], preferred_element_type=F32)

    lane = lax.broadcasted_iota(jnp.int32, (2 * HALF, 128), 1)
    low = lane < HD

    def head_pair(one, two, head):
        pair = slice((head // 2) * 128, (head // 2) * 128 + 128)
        first, second = one[:, pair], two[:, pair]
        if head % 2 == 0:
            return jnp.where(low, first, pltpu.roll(second, HD, 1))
        return jnp.where(low, pltpu.roll(first, HD, 1), second)

    values = project(loads[0], wv)
    for head in range(4):
        for half in range(2):
            kv_send[head, half, :, 128:256] = values[
                half * HALF : half * HALF + HALF, head * 128 : head * 128 + 128
            ].astype(BF16)
    key_one = project(loads[1], wk1)
    key_two = project(loads[2], wk2)
    for head in range(4):
        both = head_pair(key_one, key_two, head).astype(BF16)
        for half in range(2):
            kv_send[head, half, :, 0:128] = both[half * HALF : half * HALF + HALF]
    query_one = project(loads[3], wq1)
    query_two = project(loads[4], wq2)
    for head in range(4):
        both = (head_pair(query_one, query_two, head) * (HD**-0.5)).astype(BF16)
        for half in range(2):
            q_send[head, half] = both[half * HALF : half * HALF + HALF]

    def slot(zs, xs, cs):
        return kv_buf.at[zs, pl.ds(pl.multiple_of((xs * 2 + cs) * HALF, HALF), HALF), :]

    def slot_half(zs, xs, cs, part):
        start = pl.multiple_of((xs * 2 + cs) * HALF + part * (HALF // 2), HALF // 2)
        return kv_buf.at[zs, pl.ds(start, HALF // 2), :]

    z_sends = []
    for step in range(4):
        head = (z + step) % 4
        target = 4 * c + head
        for core in range(2):
            index = step * 2 + core
            device = {"sp": target * NX + x, "tp": core}
            kv_copy = remote(
                kv_send.at[head, core], slot(z, x, core), kv_ss.at[index], kv_rs.at[z], device
            )
            q_copy = remote(q_send.at[head, core], q_raw.at[z], q_ss.at[index], q_rs.at[z], device)
            if step == 0:
                away = jnp.logical_not((target == z) & (c == core))
            else:
                away = jnp.logical_not((target == z) & (c == core))
            z_sends.append((away, kv_copy, q_copy))

            @pl.when(away)
            def _(kv_copy=kv_copy, q_copy=q_copy):
                kv_copy.start()
                q_copy.start()

    own_head = z % 4
    local = src_tp == c

    @pl.when(local)
    def _():
        kv_buf[z, pl.ds(pl.multiple_of((x * 2 + c) * HALF, HALF), HALF), :] = kv_send[own_head, c]
        q_raw[z] = q_send[own_head, c]

    glu_value = project(loads[5], wgv).astype(BF16).astype(F32)
    glu_gate = project(loads[6], wgg).astype(BF16).astype(F32)
    gated = (glu_value * jax.nn.sigmoid(glu_gate)).astype(BF16)
    halo_send[...] = gated[2 * HALF - 32 :]
    gated_ext[32:, :] = gated.astype(F32)
    halo_copy = remote(halo_send, halo_recv, halo_sem.at[0], halo_sem.at[1], following)
    halo_copy.start()
    pending.append(halo_copy)

    taps = ck_ref[...]

    def conv_chunk(part):
        base = part * 32
        total = None
        for shift in range(8):
            partial = None
            span = 32 if shift == 0 else 40
            for group in range(5):
                tap = 8 * group + shift - 2
                if tap < 0 or tap >= CW:
                    continue
                term = taps[tap : tap + 1, :] * gated_ext[base + 8 * group : base + 8 * group + span, :]
                partial = term if partial is None else partial + term
            moved = partial[shift : shift + 32, :]
            total = moved if total is None else total + moved
        convd[base : base + 32, :] = total
        sums = jnp.sum(total, axis=-1, keepdims=True)
        squares = jnp.sum(total * total, axis=-1, keepdims=True)
        sums_send[base : base + 32, :] = jnp.where(low[:32], sums, squares)

    def stage_one(zs):
        copies = (
            remote(slot(zs, x, c), slot(zs, x, c), xs_ss.at[0, zs], xs_rs.at[0, zs], right),
            remote(slot(zs, x, c), slot(zs, x, c), xs_ss.at[1, zs], xs_rs.at[1, zs], left),
            remote(slot(zs, x, c), slot(zs, x, c), d_ss.at[0, zs], d_rs.at[0, zs], partner),
        )

        @pl.when(jnp.logical_not((zs == z) & local))
        def _():
            remote(slot(zs, x, c), slot(zs, x, c), kv_ss.at[0], kv_rs.at[zs], partner).wait_recv()

        for copy in copies:
            copy.start()
        pending.extend(copies)

    def stage_two(zs):
        remote(slot(zs, xl, c), slot(zs, xl, c), xs_ss.at[0, zs], xs_rs.at[0, zs], right).wait_recv()
        copies = (
            remote(
                slot_half(zs, xl, c, 0), slot_half(zs, xl, c, 0), xs_ss.at[2, zs], xs_rs.at[2, zs], right
            ),
            remote(slot(zs, xl, c), slot(zs, xl, c), d_ss.at[1, zs], d_rs.at[1, zs], partner),
        )
        for copy in copies:
            copy.start()
        pending.extend(copies)
        remote(slot(zs, xr, c), slot(zs, xr, c), xs_ss.at[1, zs], xs_rs.at[1, zs], left).wait_recv()
        copies = (
            remote(
                slot_half(zs, xr, c, 1), slot_half(zs, xr, c, 1), xs_ss.at[3, zs], xs_rs.at[3, zs], left
            ),
            remote(slot(zs, xr, c), slot(zs, xr, c), d_ss.at[2, zs], d_rs.at[2, zs], partner),
        )
        for copy in copies:
            copy.start()
        pending.extend(copies)

    def stage_three(zs):
        for part in range(2):
            remote(
                slot_half(zs, xo, c, part),
                slot_half(zs, xo, c, part),
                xs_ss.at[2 + part, zs],
                xs_rs.at[2 + part, zs],
                right,
            ).wait_recv()
        copy = remote(slot(zs, xo, c), slot(zs, xo, c), d_ss.at[3, zs], d_rs.at[3, zs], partner)
        copy.start()
        pending.append(copy)

    def w_wait(kind, side):
        source = yl if side == 0 else yr
        ref = w_buf.at[source, c, kind]
        remote(ref, ref, w_ss.at[side, kind], w_rs.at[side, kind], up).wait_recv()
        return ref

    def w_share(source, kind, relation):
        ref = w_buf.at[source, c, kind]
        copy = remote(ref, ref, wd_ss.at[relation, kind], wd_rs.at[relation, kind], partner)
        copy.start()
        return copy

    order = [(z + offset) % NZ for offset in Z_ORDER]
    for step in range(NZ + 2):
        if step < NZ:
            stage_one(order[step])
        if step == 0:
            halo_copy.wait_recv()
            rows = halo_recv[...].astype(F32)
            gated_ext[0:32, :] = jnp.where(me == 0, jnp.zeros_like(rows), rows)
        if 0 <= step - 1 < NZ:
            stage_two(order[step - 1])
        if 0 <= step - 2 < NZ:
            stage_three(order[step - 2])
        if step < NZ:
            conv_chunk(step)
        if step == NZ:
            sums_copy = remote(sums_send, sums_recv, sums_sem.at[0], sums_sem.at[1], partner)
            sums_copy.start()
            pending.append(sums_copy)

    for kind in range(2):
        own_w[kind].wait()
        pending.append(w_share(y, kind, 0))
    ref = w_wait(0, 0)
    copy = remote(ref, ref, w_ss.at[2, 0], w_rs.at[2, 0], up)
    copy.start()
    pending.append(copy)
    pending.append(w_share(yl, 0, 1))
    ref = w_wait(1, 1)
    copy = remote(ref, ref, w_ss.at[2, 1], w_rs.at[2, 1], down)
    copy.start()
    pending.append(copy)
    pending.append(w_share(yr, 1, 2))

    sums_copy.wait_recv()
    lam_copy.wait_recv()
    for half in range(2):
        rows = slice(half * HALF, half * HALF + HALF)
        row_sums = sums_send[rows, :] + sums_recv[rows, :]
        mean = row_sums[:, 0:1] * (1.0 / DC)
        square = row_sums[:, HD : HD + 1] * (1.0 / DC)
        scaled = (convd[rows, :] - mean) * lax.rsqrt(square - mean * mean + EPSILON) * cg_ref[...]
        result = (scaled * jax.nn.sigmoid(scaled)).astype(BF16)

        @pl.when(c == half)
        def _(result=result):
            conv_full[c] = result

        @pl.when(c != half)
        def _(result=result):
            conv_send[...] = result

    conv_copy = remote(conv_send, conv_full.at[c], cx_sem.at[0], cx_sem.at[1], partner)
    conv_copy.start()
    pending.append(conv_copy)

    for zs in range(NZ):

        @pl.when(jnp.logical_not((zs == z) & local))
        def _(zs=zs):
            remote(q_raw.at[zs], q_raw.at[zs], q_ss.at[0], q_rs.at[zs], partner).wait_recv()

        rows = q_raw[zs]
        zero = jnp.zeros_like(rows)
        low_half = low[:HALF]
        qs[zs, :HALF] = jnp.where(low_half, rows, zero)
        qs[zs, HALF:] = jnp.where(low_half, zero, rows)
    m_buf[...] = jnp.full_like(m_buf, NEG_FILL)
    acc[...] = jnp.zeros_like(acc)

    ones = jnp.ones((NX * 2 * HALF, 128), BF16)
    head_row = jnp.where(local, lam_ref[pl.ds(own_head, 1), :], lam_recv[pl.ds(own_head, 1), :])

    def tile(s, zt, diagonal):
        keys = kv_buf[s, :, 0:128]
        scores = lax.dot_general(
            qs[zt], keys, (((1,), (1,)), ((), ())), preferred_element_type=F32
        )
        if diagonal:
            row = lax.broadcasted_iota(jnp.int32, scores.shape, 0)
            col = lax.broadcasted_iota(jnp.int32, scores.shape, 1)
            query_segment = (x * 4 + c * 2) + ((row & (HALF - 1)) >> 6)
            scores = jnp.where((col >> 6) <= query_segment, scores, NEG_FILL)
        old = m_buf[zt]
        new = jnp.maximum(old, jnp.max(scores, axis=-1, keepdims=True))
        weights = jnp.exp(scores - jnp.concatenate([new] * 8, axis=1))
        factor = jnp.exp(old - new)
        rhs = jnp.concatenate([kv_buf[s, :, 128:256], ones], axis=1)
        part = jnp.dot(weights.astype(BF16), rhs, preferred_element_type=F32)
        acc[zt] = acc[zt] * jnp.concatenate([factor, factor], axis=1) + part
        m_buf[zt] = new

    def ret_copy(s):
        return remote(
            ret_send.at[s], attn_buf.at[z], ret_ss.at[s], ret_rs.at[z], {"sp": s * NX + x}
        )

    def log_copy(s):
        return remote(
            lsend.at[s], log_buf.at[own_head, c], log_ss.at[s], log_rs.at[own_head, c],
            {"sp": s * NX + x, "tp": src_tp},
        )

    def advance(s, carry):
        for relation, xs in enumerate((x, xl, xr, xo)):
            xs_o = xs
            ref = slot(s, xs_o, other)
            remote(ref, ref, d_ss.at[relation, s], d_rs.at[relation, s], partner).wait_recv()
        tile(s, s, True)
        pooled = acc[s]
        sums = pooled[:, 128:256]
        normal = pooled[:, 0:128] / sums
        head_out = normal[:HALF] - head_row * normal[HALF:]
        head_out = (
            head_out
            * lax.rsqrt(jnp.mean(head_out * head_out, axis=-1, keepdims=True) + EPSILON)
            * hg_ref[...]
            * HEAD_SCALE
        ).astype(BF16)
        logs = m_buf[s] + jnp.log(sums)
        first = jnp.transpose(logs[:HALF])[0:8]
        second = jnp.transpose(logs[HALF:])[0:8]
        sub = lax.broadcasted_iota(jnp.int32, (8, 128), 0)
        log_rows = jnp.where(sub == 0, first, second)
        ret_send[s] = head_out
        lsend[s] = log_rows

        @pl.when(s == z)
        def _():
            attn_buf[z] = head_out

        @pl.when((s == z) & local)
        def _():
            log_buf[own_head, c] = log_rows

        @pl.when(s != z)
        def _():
            ret_copy(s).start()

        @pl.when(jnp.logical_not((s == z) & local))
        def _():
            log_copy(s).start()

        def inner(zt, inner_carry):
            tile(s, zt, False)
            return inner_carry

        return lax.fori_loop(s + 1, NZ, inner, carry)

    lax.fori_loop(0, NZ, advance, 0)

    w_wait(1, 0)
    pending.append(w_share(yl, 1, 1))
    w_wait(0, 1)
    pending.append(w_share(yr, 0, 2))
    for kind in range(2):
        ref = w_buf.at[yo, c, kind]
        remote(ref, ref, w_ss.at[2, kind], w_rs.at[2, kind], up).wait_recv()
        pending.append(w_share(yo, kind, 3))
    conv_copy.wait_recv()
    for kind in range(2):
        for relation, source in enumerate((y, yl, yr, yo)):
            ref = w_buf.at[source, other, kind]
            remote(ref, ref, wd_ss.at[relation, kind], wd_rs.at[relation, kind], partner).wait_recv()

    for quarter in range(NY):
        cols = slice(quarter * 512, quarter * 512 + 512)
        acc_out[:, cols] = jnp.dot(
            conv_full[0], w_buf[quarter, 0, 0], preferred_element_type=F32
        ) + jnp.dot(conv_full[1], w_buf[quarter, 1, 0], preferred_element_type=F32)

    for hs in range(NZ):

        @pl.when(hs != z)
        def _(hs=hs):
            remote(
                attn_buf.at[hs], attn_buf.at[hs], ret_ss.at[hs], ret_rs.at[hs], partner
            ).wait_recv()

    sides = [jnp.concatenate([attn_buf[4 * side + k] for k in range(4)], axis=1) for side in range(2)]
    for quarter in range(NY):
        cols = slice(quarter * 512, quarter * 512 + 512)
        result = acc_out[:, cols]
        for side in range(2):
            result = result + jnp.dot(
                sides[side], w_buf[quarter, side, 1], preferred_element_type=F32
            )
        out_ref[:, cols] = result.astype(BF16)

    for head in range(4):
        for half in range(2):
            from_self = (4 * c + head == z) & (c == half)

            @pl.when(jnp.logical_not(from_self))
            def _(head=head, half=half):
                ref = log_buf.at[head, half]
                remote(ref, ref, log_ss.at[0], log_rs.at[head, half], partner).wait_recv()

            for which in range(2):
                log_ref[which, head : head + 1, half * HALF : half * HALF + HALF] = log_buf[
                    head, half, which : which + 1, :
                ]

    for away, kv_copy, q_copy in z_sends:

        @pl.when(away)
        def _(kv_copy=kv_copy, q_copy=q_copy):
            kv_copy.wait_send()
            q_copy.wait_send()

    for copy in pending:
        copy.wait_send()
    for s in range(NZ):

        @pl.when(s != z)
        def _(s=s):
            ret_copy(s).wait_send()

        @pl.when(jnp.logical_not((s == z) & local))
        def _(s=s):
            log_copy(s).wait_send()


def body(
    inputs,
    norm_gain,
    w_glu_value,
    w_glu_gate,
    w_query_one,
    w_query_two,
    w_key_one,
    w_key_two,
    w_value,
    conv_kernel,
    conv_gain,
    head_gain,
    lambda_head,
    w_out_conv,
    w_out_attn,
):
    lam = jnp.broadcast_to(jnp.pad(lambda_head, (0, 4))[:, None], (8, 128))
    vmem = pl.BlockSpec(memory_space=pltpu.VMEM)
    hbm = pl.BlockSpec(memory_space=pl.ANY)
    dma = pltpu.SemaphoreType.DMA
    mixed, logs = pl.pallas_call(
        kernel,
        out_shape=(
            jax.ShapeDtypeStruct((HALF, D), BF16),
            jax.ShapeDtypeStruct((2, 4, 2 * HALF), F32),
        ),
        in_specs=[vmem] * 6 + [hbm] * 9,
        out_specs=(vmem, vmem),
        scratch_shapes=[
            pltpu.VMEM((D, 512), BF16),
            pltpu.VMEM((D, 512), BF16),
            pltpu.VMEM((D, 256), BF16),
            pltpu.VMEM((D, 256), BF16),
            pltpu.VMEM((D, 256), BF16),
            pltpu.VMEM((D, 256), BF16),
            pltpu.VMEM((D, 512), BF16),
            pltpu.VMEM((2 * HALF, D), BF16),
            pltpu.VMEM((4, 2, HALF, 256), BF16),
            pltpu.VMEM((4, 2, HALF, 128), BF16),
            pltpu.VMEM((NZ, NX * 2 * HALF, 256), BF16),
            pltpu.VMEM((NZ, HALF, 128), BF16),
            pltpu.VMEM((NZ, 2 * HALF, 128), BF16),
            pltpu.VMEM((2 * HALF + 32, 512), F32),
            pltpu.VMEM((32, 512), BF16),
            pltpu.VMEM((32, 512), BF16),
            pltpu.VMEM((2 * HALF, 512), F32),
            pltpu.VMEM((2 * HALF, 128), F32),
            pltpu.VMEM((2 * HALF, 128), F32),
            pltpu.VMEM((2, HALF, 512), BF16),
            pltpu.VMEM((HALF, 512), BF16),
            pltpu.VMEM((NZ, 2 * HALF, 128), F32),
            pltpu.VMEM((NZ, 2 * HALF, 256), F32),
            pltpu.VMEM((NZ, HALF, 128), BF16),
            pltpu.VMEM((NZ, HALF, 128), BF16),
            pltpu.VMEM((NZ, 8, 128), F32),
            pltpu.VMEM((4, 2, 8, 128), F32),
            pltpu.VMEM((8, 128), F32),
            pltpu.VMEM((NY, 2, 2, 512, 512), BF16),
            pltpu.VMEM((HALF, D), F32),
            dma((7,)),
            dma((2,)),
            dma((8,)),
            dma((8,)),
            dma((NZ,)),
            dma((NZ,)),
            dma((4, NZ)),
            dma((4, NZ)),
            dma((4, NZ)),
            dma((4, NZ)),
            dma((2,)),
            dma((2,)),
            dma((2,)),
            dma((2,)),
            dma((NZ,)),
            dma((NZ,)),
            dma((NZ,)),
            dma((4, 2)),
            dma((3, 2)),
            dma((3, 2)),
            dma((4, 2)),
            dma((4, 2)),
            dma((2,)),
        ],
        compiler_params=pltpu.CompilerParams(
            collective_id=0, has_side_effects=True, vmem_limit_bytes=60 * 1024 * 1024
        ),
        name="mixer",
    )(
        inputs[0],
        norm_gain[None],
        conv_kernel.astype(F32),
        conv_gain[None],
        head_gain[None],
        lam,
        w_glu_value,
        w_glu_gate,
        w_query_one,
        w_query_two,
        w_key_one,
        w_key_two,
        w_value,
        w_out_conv,
        w_out_attn,
    )
    return (mixed[None], logs[None])


def solution(mesh):
    return jax.shard_map(
        body,
        mesh=mesh,
        in_specs=(
            P("fs", ("sp", "tp"), None),
            P(),
            P(None, "tp"),
            P(None, "tp"),
            P(None, "tp"),
            P(None, "tp"),
            P(None, "tp"),
            P(None, "tp"),
            P(None, "tp"),
            P(None, "tp"),
            P("tp"),
            P(),
            P("tp"),
            P("tp", "fs"),
            P("tp", "fs"),
        ),
        out_specs=(P("fs", ("sp", "tp"), None), P("fs", None, "tp", "sp")),
        check_vma=False,
    )
```

```python
import jax
import jax.numpy as jnp
from jax import lax
from jax.experimental import pallas as pl
from jax.experimental.pallas import tpu as pltpu
from jax.sharding import PartitionSpec as P

D = 2048
DC = 1024
HD = 64
CW = 31
NZ = 8
NX = 4
NY = 4
HALF = 128
NEG_FILL = -1e30
EPSILON = 1e-05
HEAD_SCALE = 0.8
MESH = pl.DeviceIdType.MESH
F32 = jnp.float32
BF16 = jnp.bfloat16
W_ONE = 5
W_TWO = 8


def remote(src, dst, send_sem, recv_sem, device):
    return pltpu.make_async_remote_copy(
        src_ref=src,
        dst_ref=dst,
        send_sem=send_sem,
        recv_sem=recv_sem,
        device_id=device,
        device_id_type=MESH,
    )


def kernel(
    x_ref,
    gain_ref,
    ck_ref,
    cg_ref,
    hg_ref,
    lam_ref,
    wgv_hbm,
    wgg_hbm,
    wq1_hbm,
    wq2_hbm,
    wk1_hbm,
    wk2_hbm,
    wv_hbm,
    woc_hbm,
    woa_hbm,
    out_ref,
    log_ref,
    wgv,
    wgg,
    wq1,
    wq2,
    wk1,
    wk2,
    wv,
    normed,
    kv_send,
    q_send,
    kv_buf,
    q_raw,
    qs,
    gated_ext,
    halo_send,
    halo_recv,
    convd,
    sums_send,
    sums_recv,
    conv_full,
    conv_send,
    m_buf,
    acc,
    score_a,
    score_b,
    max_a,
    max_b,
    bias,
    gain_t,
    ret_send,
    attn_buf,
    lsend,
    log_buf,
    lam_own,
    lam_recv,
    w_buf,
    acc_out,
    load_sem,
    norm_sem,
    kv_ss,
    q_ss,
    kv_rs,
    q_rs,
    xs_ss,
    xs_rs,
    d_ss,
    d_rs,
    halo_sem,
    sums_sem,
    cx_sem,
    lam_sem,
    ret_ss,
    ret_rs,
    log_ss,
    log_rs,
    w_ss,
    w_rs,
    wx_ss,
    wx_rs,
    wd_ss,
    wd_rs,
    wp_ss,
    wp_rs,
    own_sem,
):
    me = lax.axis_index("sp")
    y = lax.axis_index("fs")
    c = lax.axis_index("tp")
    z, x = me // NX, me % NX
    other = 1 - c
    xr, xl, xo = (x + 1) % NX, (x + 3) % NX, (x + 2) % NX
    yr, yl, yo = (y + 1) % NY, (y + 3) % NY, (y + 2) % NY
    src_tp = z // 4
    own_head = z % 4
    local = src_tp == c
    partner = {"tp": other}
    right = {"sp": z * NX + xr}
    left = {"sp": z * NX + xl}
    up = {"fs": yr}
    down = {"fs": yl}
    following = {"sp": (me + 1) % (NZ * NX)}
    preceding = {"sp": (me + NZ * NX - 1) % (NZ * NX)}
    pending = []

    def begin(copy):
        copy.start()
        pending.append(copy)
        return copy

    loads = []
    for index, (src, dst) in enumerate(
        ((wv_hbm, wv), (wk1_hbm, wk1), (wk2_hbm, wk2), (wq1_hbm, wq1), (wq2_hbm, wq2),
         (wgv_hbm, wgv), (wgg_hbm, wgg))
    ):
        loads.append(pltpu.make_async_copy(src, dst, load_sem.at[index]))
        loads[-1].start()

    barrier = pltpu.get_barrier_semaphore()
    for device in (partner, right, left, up, down, following, preceding):
        pl.semaphore_signal(barrier, inc=1, device_id=device, device_id_type=MESH)
    for step in range(1, NZ):
        for core in range(2):
            pl.semaphore_signal(
                barrier,
                inc=1,
                device_id={"sp": ((z + step) % NZ) * NX + x, "tp": core},
                device_id_type=MESH,
            )

    my_rows = pl.multiple_of(c * HALF, HALF)
    peer_rows = pl.multiple_of(other * HALF, HALF)
    for part in range(4):
        rows_f = x_ref[part * 32 : part * 32 + 32, :].astype(F32)
        scale = lax.rsqrt(jnp.mean(rows_f * rows_f, axis=-1, keepdims=True) + EPSILON)
        normed[pl.ds(my_rows + part * 32, 32), :] = (rows_f * scale * gain_ref[...]).astype(BF16)

    lane = lax.broadcasted_iota(jnp.int32, (HALF, 128), 1)
    low = lane < HD

    def head_pair(one, two, head):
        pair = slice((head // 2) * 128, (head // 2) * 128 + 128)
        first, second = one[:, pair], two[:, pair]
        if head % 2 == 0:
            return jnp.where(low, first, pltpu.roll(second, HD, 1))
        return jnp.where(low, pltpu.roll(first, HD, 1), second)

    def project_qkv(rows, half, fresh):
        block = normed[pl.ds(rows, HALF), :]

        def project(index, weight):
            if fresh:
                loads[index].wait()
            return jnp.dot(block, weight[...], preferred_element_type=F32)

        values = project(0, wv)
        for head in range(4):
            kv_send[head, half, :, 128:256] = jnp.transpose(
                values[:, head * 128 : head * 128 + 128]
            ).astype(BF16)
        key_one = project(1, wk1)
        key_two = project(2, wk2)
        for head in range(4):
            kv_send[head, half, :, 0:128] = head_pair(key_one, key_two, head).astype(BF16)
        query_one = project(3, wq1)
        query_two = project(4, wq2)
        for head in range(4):
            q_send[head, half] = (head_pair(query_one, query_two, head) * (HD**-0.5)).astype(BF16)

    def project_glu(rows, fresh):
        block = normed[pl.ds(rows, HALF), :]
        if fresh:
            loads[5].wait()
            loads[6].wait()
        value = jnp.dot(block, wgv[...], preferred_element_type=F32).astype(BF16).astype(F32)
        gate = jnp.dot(block, wgg[...], preferred_element_type=F32).astype(BF16).astype(F32)
        gated = (value * jax.nn.sigmoid(gate)).astype(BF16)
        gated_ext[pl.ds(pl.multiple_of(rows + 32, 32), HALF), :] = gated.astype(F32)

    project_qkv(my_rows, c, True)
    for index in range(4):
        lam_own[index : index + 1, :] = jnp.full((1, 128), lam_ref[index], F32)
    lam_own[4:8, :] = jnp.zeros((4, 128), F32)

    pl.semaphore_wait(barrier, 7 + 2 * (NZ - 1))

    mine = normed.at[pl.ds(my_rows, HALF), :]
    norm_copy = begin(remote(mine, mine, norm_sem.at[0], norm_sem.at[1], partner))

    def slot(zs, xs, cs):
        return kv_buf.at[zs, pl.ds(pl.multiple_of((xs * 2 + cs) * HALF, HALF), HALF), :]

    def slot_half(zs, xs, cs, part):
        start = pl.multiple_of((xs * 2 + cs) * HALF + part * (HALF // 2), HALF // 2)
        return kv_buf.at[zs, pl.ds(start, HALF // 2), :]

    u = z % 4
    ranks = (u, u + 1 - 2 * (u % 2), 2 - u // 2, 3 * (1 - u // 2))
    same = 1 - src_tp - c + 2 * src_tp * c
    z_sends = []

    def z_send(rank, half, index):
        head = same * ranks[rank] + (1 - same) * ranks[3 - rank]
        target = 4 * c + head
        device = {"sp": target * NX + x, "tp": half}
        kv_copy = remote(
            kv_send.at[head, half], slot(z, x, half), kv_ss.at[index], kv_rs.at[z], device
        )
        q_copy = remote(q_send.at[head, half], q_raw.at[z], q_ss.at[index], q_rs.at[z], device)
        away = jnp.logical_not((target == z) & (half == c))
        z_sends.append((away, kv_copy, q_copy))

        @pl.when(away)
        def _():
            kv_copy.start()
            q_copy.start()

    z_send(0, c, 0)
    z_send(1, c, 1)

    @pl.when(local)
    def _():
        kv_buf[z, pl.ds(pl.multiple_of((x * 2 + c) * HALF, HALF), HALF), :] = kv_send[own_head, c]
        q_raw[z] = q_send[own_head, c]

    w_hbm = (woc_hbm, woa_hbm)

    def w_own(side, kind, device):
        begin(remote(w_hbm[kind], w_buf.at[y, c, kind], w_ss.at[side, kind], w_rs.at[side, kind], device))

    w_own(0, 0, up)
    w_own(1, 1, down)
    lam_copy = begin(remote(lam_own, lam_recv, lam_sem.at[0], lam_sem.at[1], partner))

    project_glu(my_rows, True)
    norm_copy.wait_recv()
    project_qkv(peer_rows, other, False)
    z_send(0, other, 2)
    z_send(1, other, 3)
    z_send(2, c, 4)
    z_send(2, other, 5)
    z_send(3, c, 6)
    z_send(3, other, 7)
    project_glu(peer_rows, False)
    halo_send[...] = gated_ext[2 * HALF :, :].astype(BF16)
    halo_copy = begin(remote(halo_send, halo_recv, halo_sem.at[0], halo_sem.at[1], following))

    own_w = []
    for kind in range(2):
        own = pltpu.make_async_copy(w_hbm[kind], w_buf.at[y, c, kind], own_sem.at[kind])
        own.start()
        own_w.append(own)
        begin(remote(w_hbm[kind], w_buf.at[y, c, kind], wd_ss.at[0, kind], wd_rs.at[0, kind], partner))

    taps = ck_ref[...].astype(F32)

    def conv_chunk(part):
        base = part * 32
        total = None
        for shift in range(8):
            partial = None
            span = 32 if shift == 0 else 40
            for group in range(5):
                tap = 8 * group + shift - 2
                if tap < 0 or tap >= CW:
                    continue
                term = taps[tap : tap + 1, :] * gated_ext[base + 8 * group : base + 8 * group + span, :]
                partial = term if partial is None else partial + term
            moved = partial[shift : shift + 32, :]
            total = moved if total is None else total + moved
        convd[base : base + 32, :] = total
        sums = jnp.sum(total, axis=-1, keepdims=True)
        squares = jnp.sum(total * total, axis=-1, keepdims=True)
        sums_send[base : base + 32, :] = jnp.where(low[:32], sums, squares)

    def stage_one(zs):
        ref = slot(zs, x, c)
        away = jnp.logical_not((zs == z) & local)

        @pl.when(away)
        def _():
            remote(ref, ref, kv_ss.at[0], kv_rs.at[zs], partner).wait_recv()

        begin(remote(ref, ref, xs_ss.at[0, zs], xs_rs.at[0, zs], right))
        begin(remote(ref, ref, xs_ss.at[1, zs], xs_rs.at[1, zs], left))
        begin(remote(ref, ref, d_ss.at[0, zs], d_rs.at[0, zs], partner))

        @pl.when(away)
        def _():
            remote(q_raw.at[zs], q_raw.at[zs], q_ss.at[0], q_rs.at[zs], partner).wait_recv()

        rows = q_raw[zs]
        zero = jnp.zeros_like(rows)
        qs[zs, :HALF] = jnp.where(low, rows, zero)
        qs[zs, HALF:] = jnp.where(low, zero, rows)

    def stage_two(zs):
        ref = slot(zs, xl, c)
        remote(ref, ref, xs_ss.at[0, zs], xs_rs.at[0, zs], right).wait_recv()
        part = slot_half(zs, xl, c, 0)
        begin(remote(part, part, xs_ss.at[2, zs], xs_rs.at[2, zs], right))
        begin(remote(ref, ref, d_ss.at[1, zs], d_rs.at[1, zs], partner))
        ref = slot(zs, xr, c)
        remote(ref, ref, xs_ss.at[1, zs], xs_rs.at[1, zs], left).wait_recv()
        part = slot_half(zs, xr, c, 1)
        begin(remote(part, part, xs_ss.at[3, zs], xs_rs.at[3, zs], left))
        begin(remote(ref, ref, d_ss.at[2, zs], d_rs.at[2, zs], partner))

    def stage_three(zs):
        for part in range(2):
            ref = slot_half(zs, xo, c, part)
            remote(ref, ref, xs_ss.at[2 + part, zs], xs_rs.at[2 + part, zs], right).wait_recv()
        ref = slot(zs, xo, c)
        begin(remote(ref, ref, d_ss.at[3, zs], d_rs.at[3, zs], partner))

    def stage_four(zs):
        for relation, xs in enumerate((x, xl, xr, xo)):
            ref = slot(zs, xs, other)
            remote(ref, ref, d_ss.at[relation, zs], d_rs.at[relation, zs], partner).wait_recv()

    def w_wait(source, kind, side):
        ref = w_buf.at[source, c, kind]
        remote(ref, ref, w_ss.at[side, kind], w_rs.at[side, kind], up).wait_recv()

    def w_share(source, kind, relation):
        ref = w_buf.at[source, c, kind]
        begin(remote(ref, ref, wd_ss.at[relation, kind], wd_rs.at[relation, kind], partner))

    def piece(source, core, kind, xs):
        return w_buf.at[source, core, kind, pl.ds(pl.multiple_of(xs * 128, 128), 128), :]

    def piece_share(kind, relation, xs):
        ref = piece(yo, c, kind, xs)
        begin(remote(ref, ref, wp_ss.at[relation, kind], wp_rs.at[relation, kind], partner))

    def w_one():
        w_wait(yl, 0, 0)
        ref = piece(yl, c, 0, x)
        begin(remote(ref, ref, w_ss.at[2, 0], w_rs.at[2, 0], up))
        w_own(0, 1, up)
        w_wait(yr, 1, 1)
        ref = piece(yr, c, 1, x)
        begin(remote(ref, ref, w_ss.at[2, 1], w_rs.at[2, 1], down))
        w_own(1, 0, down)
        w_share(yl, 0, 1)
        w_share(yr, 1, 2)

    def w_two():
        for kind in range(2):
            ref = piece(yo, c, kind, x)
            remote(ref, ref, w_ss.at[2, kind], w_rs.at[2, kind], up).wait_recv()
            begin(remote(ref, ref, wx_ss.at[0, kind], wx_rs.at[0, kind], right))
            begin(remote(ref, ref, wx_ss.at[1, kind], wx_rs.at[1, kind], left))
            piece_share(kind, 0, x)

    def w_three():
        for kind in range(2):
            for side, xs in ((0, xl), (1, xr)):
                ref = piece(yo, c, kind, xs)
                remote(ref, ref, wx_ss.at[side, kind], wx_rs.at[side, kind], right).wait_recv()
                if side == kind:
                    device = right if side == 0 else left
                    begin(remote(ref, ref, wx_ss.at[2, kind], wx_rs.at[2, kind], device))
                piece_share(kind, 1 + side, xs)

    def w_four():
        w_wait(yl, 1, 0)
        w_share(yl, 1, 1)
        w_wait(yr, 0, 1)
        w_share(yr, 0, 2)
        for kind in range(2):
            ref = piece(yo, c, kind, xo)
            remote(ref, ref, wx_ss.at[2, kind], wx_rs.at[2, kind], right).wait_recv()
            piece_share(kind, 3, xo)

    def w_five(kind):
        for relation, source in enumerate((y, yl, yr)):
            ref = w_buf.at[source, other, kind]
            remote(ref, ref, wd_ss.at[relation, kind], wd_rs.at[relation, kind], partner).wait_recv()
        for relation, xs in enumerate((x, xl, xr, xo)):
            ref = piece(yo, other, kind, xs)
            remote(ref, ref, wp_ss.at[relation, kind], wp_rs.at[relation, kind], partner).wait_recv()

    def conv_finish():
        sums_copy.wait_recv()
        for half in range(2):
            rows = slice(half * HALF, half * HALF + HALF)
            row_sums = sums_send[rows, :] + sums_recv[rows, :]
            mean = row_sums[:, 0:1] * (1.0 / DC)
            square = row_sums[:, HD : HD + 1] * (1.0 / DC)
            scaled = (convd[rows, :] - mean) * lax.rsqrt(square - mean * mean + EPSILON) * cg_ref[...]
            result = (scaled * jax.nn.sigmoid(scaled)).astype(BF16)

            @pl.when(c == half)
            def _(result=result):
                conv_full[c] = result

            @pl.when(c != half)
            def _(result=result):
                conv_send[...] = result

        return begin(remote(conv_send, conv_full.at[c], cx_sem.at[0], cx_sem.at[1], partner))

    m_buf[...] = jnp.full_like(m_buf, NEG_FILL)
    acc[...] = jnp.zeros_like(acc)
    bias[0] = jnp.zeros((16, 8, 256), F32)
    query_segment = (x * 4 + c * 2) + (
        (lax.broadcasted_iota(jnp.int32, (8, 256), 1) & (HALF - 1)) >> 6
    )
    for segment in range(16):
        bias[1, segment] = jnp.where(query_segment >= segment, 0.0, NEG_FILL)
    gain_t[...] = jnp.transpose(jnp.broadcast_to(hg_ref[...], (128, 128))) * HEAD_SCALE

    def place(index):
        odd = index % 2
        offset = odd * ((index + 1) // 2) + (1 - odd) * (NZ - index // 2)
        return (z + offset) % NZ

    def which(t):
        i = 0
        for bound in (1, 3, 6, 10, 15, 21, 28):
            i = i + jnp.where(t >= bound, 1, 0)
        j = t - (i * (i + 1)) // 2
        zi, zj = place(i), place(j)
        return jnp.minimum(zi, zj), jnp.maximum(zi, zj), (j + 1) // (i + 1)

    def scores(t, score_ref, max_ref):
        s, zt, kind = which(t)
        queries = qs[zt]
        best = None
        for start in range(0, 1024, 256):
            block = lax.dot_general(
                kv_buf[s, start : start + 256, 0:128],
                queries,
                (((1,), (1,)), ((), ())),
                preferred_element_type=F32,
            )
            score_ref[start : start + 256] = block
            for inner in range(4):
                top = None
                for row in range(inner * 64, inner * 64 + 64, 8):
                    top = block[row : row + 8] if top is None else jnp.maximum(top, block[row : row + 8])
                top = top + bias[kind, start // 64 + inner]
                best = top if best is None else jnp.maximum(best, top)
        max_ref[...] = best

    ones = jnp.ones((16, 256), BF16)

    def absorb(t, score_ref, max_ref):
        s, zt, kind = which(t)
        old = m_buf[zt, 0:1]
        new = jnp.maximum(old, jnp.max(max_ref[...], axis=0, keepdims=True))
        factor = jnp.exp(old - new)
        total = None
        for start in range(0, 1024, 256):
            weights = []
            for inner in range(4):
                row = start + inner * 64
                shifted = new - bias[kind, row // 64, 0:1]
                weights.append(jnp.exp(score_ref[row : row + 64] - shifted).astype(BF16))
            lhs = jnp.concatenate(
                [
                    jnp.concatenate(
                        [
                            kv_buf[s, start : start + 128, 128:256],
                            kv_buf[s, start + 128 : start + 256, 128:256],
                        ],
                        axis=1,
                    ),
                    ones,
                ],
                axis=0,
            )
            part = jnp.dot(lhs, jnp.concatenate(weights, axis=0), preferred_element_type=F32)
            total = part if total is None else total + part
        acc[zt] = acc[zt] * factor + total
        m_buf[zt] = jnp.broadcast_to(new, (8, 256))

    def ret_copy(s):
        return remote(
            ret_send.at[s], attn_buf.at[z], ret_ss.at[s], ret_rs.at[z], {"sp": s * NX + x}
        )

    def log_copy(s):
        return remote(
            lsend.at[s], log_buf.at[own_head, c], log_ss.at[s], log_rs.at[own_head, c],
            {"sp": s * NX + x, "tp": src_tp},
        )

    def finish(s):
        sums = acc[s, 128:129, :]
        normal = acc[s, 0:128, :] * (1.0 / sums)
        lam_row = jnp.where(local, lam_own[pl.ds(own_head, 1), :], lam_recv[pl.ds(own_head, 1), :])
        head_out = normal[:, :HALF] - lam_row * normal[:, HALF:]
        head_out = (
            head_out
            * lax.rsqrt(jnp.mean(head_out * head_out, axis=0, keepdims=True) + EPSILON)
            * gain_t[...]
        )
        head_out = jnp.transpose(head_out).astype(BF16)
        logs = m_buf[s, 0:1] + jnp.log(sums)
        sub = lax.broadcasted_iota(jnp.int32, (8, 128), 0)
        log_rows = jnp.where(sub == 0, logs[:, :HALF], logs[:, HALF:])
        ret_send[s] = head_out
        lsend[s] = log_rows

        @pl.when(s == z)
        def _():
            attn_buf[z] = head_out

        @pl.when((s == z) & local)
        def _():
            log_buf[own_head, c] = log_rows

        @pl.when(s != z)
        def _():
            ret_copy(s).start()

        @pl.when(jnp.logical_not((s == z) & local))
        def _():
            log_copy(s).start()

    def pair(p, carry):
        scores(2 * p + 1, score_b, max_b)
        absorb(2 * p, score_a, max_a)
        scores(2 * p + 2, score_a, max_a)
        absorb(2 * p + 1, score_b, max_b)
        return carry

    last = place(NZ - 1)
    conv_copy = None
    done_pairs = 0
    for step in range(NZ + 2):
        if step < NZ:
            stage_one(place(step))
        if step == 0:
            for part in (1, 2, 3, 4, 5, 6, 7):
                conv_chunk(part)
            halo_copy.wait_recv()
            rows = halo_recv[...].astype(F32)
            gated_ext[0:32, :] = jnp.where(me == 0, jnp.zeros_like(rows), rows)
            conv_chunk(0)
            sums_copy = begin(remote(sums_send, sums_recv, sums_sem.at[0], sums_sem.at[1], partner))
        if 0 <= step - 1 < NZ:
            stage_two(place(step - 1))
        if step == 2:
            conv_copy = conv_finish()
        if step == NZ + 1:
            lam_copy.wait_recv()

            def early(j, carry):
                zj = place(j)

                @pl.when(zj < last)
                def _():
                    finish(zj)

                return carry

            lax.fori_loop(0, 5, early, 0)
        if 0 <= step - 2 < NZ:
            stage_three(place(step - 2))
        if step == W_ONE:
            w_one()
        if step == W_TWO:
            w_two()
        if 0 <= step - 2 < NZ:
            index = step - 2
            stage_four(place(index))
            if index == 0:
                scores(0, score_a, max_a)
            else:
                end = ((index + 1) * (index + 2) // 2 - 1) // 2
                lax.fori_loop(done_pairs, end, pair, 0)
                done_pairs = end
    scores(35, score_b, max_b)
    absorb(34, score_a, max_a)
    absorb(35, score_b, max_b)

    def late(j, carry):
        zj = place(j)

        @pl.when((j > 4) | (zj > last))
        def _():
            finish(zj)

        return carry

    lax.fori_loop(0, NZ, late, 0)

    w_three()
    w_four()
    for kind in range(2):
        own_w[kind].wait()
    conv_copy.wait_recv()
    w_five(0)
    for quarter in range(NY):
        cols = slice(quarter * 512, quarter * 512 + 512)
        acc_out[:, cols] = jnp.dot(
            conv_full[0], w_buf[quarter, 0, 0], preferred_element_type=F32
        ) + jnp.dot(conv_full[1], w_buf[quarter, 1, 0], preferred_element_type=F32)
    w_five(1)

    for hs in range(NZ):

        @pl.when(hs != z)
        def _(hs=hs):
            remote(
                attn_buf.at[hs], attn_buf.at[hs], ret_ss.at[hs], ret_rs.at[hs], partner
            ).wait_recv()

    sides = [jnp.concatenate([attn_buf[4 * side + k] for k in range(4)], axis=1) for side in range(2)]
    for quarter in range(NY):
        cols = slice(quarter * 512, quarter * 512 + 512)
        result = acc_out[:, cols]
        for side in range(2):
            result = result + jnp.dot(
                sides[side], w_buf[quarter, side, 1], preferred_element_type=F32
            )
        out_ref[:, cols] = result.astype(BF16)

    for head in range(4):
        for half in range(2):
            from_self = (4 * c + head == z) & (c == half)

            @pl.when(jnp.logical_not(from_self))
            def _(head=head, half=half):
                ref = log_buf.at[head, half]
                remote(ref, ref, log_ss.at[0], log_rs.at[head, half], partner).wait_recv()

            for which_map in range(2):
                log_ref[which_map, head : head + 1, half * HALF : half * HALF + HALF] = log_buf[
                    head, half, which_map : which_map + 1, :
                ]

    for away, kv_copy, q_copy in z_sends:

        @pl.when(away)
        def _(kv_copy=kv_copy, q_copy=q_copy):
            kv_copy.wait_send()
            q_copy.wait_send()

    for copy in pending:
        copy.wait_send()
    for s in range(NZ):

        @pl.when(s != z)
        def _(s=s):
            ret_copy(s).wait_send()

        @pl.when(jnp.logical_not((s == z) & local))
        def _(s=s):
            log_copy(s).wait_send()


def body(
    inputs,
    norm_gain,
    w_glu_value,
    w_glu_gate,
    w_query_one,
    w_query_two,
    w_key_one,
    w_key_two,
    w_value,
    conv_kernel,
    conv_gain,
    head_gain,
    lambda_head,
    w_out_conv,
    w_out_attn,
):
    vmem = pl.BlockSpec(memory_space=pltpu.VMEM)
    hbm = pl.BlockSpec(memory_space=pl.ANY)
    dma = pltpu.SemaphoreType.DMA
    mixed, logs = pl.pallas_call(
        kernel,
        out_shape=(
            jax.ShapeDtypeStruct((HALF, D), BF16),
            jax.ShapeDtypeStruct((2, 4, 2 * HALF), F32),
        ),
        in_specs=[vmem] * 5 + [pl.BlockSpec(memory_space=pltpu.SMEM)] + [hbm] * 9,
        out_specs=(vmem, vmem),
        scratch_shapes=[
            pltpu.VMEM((D, 512), BF16),
            pltpu.VMEM((D, 512), BF16),
            pltpu.VMEM((D, 256), BF16),
            pltpu.VMEM((D, 256), BF16),
            pltpu.VMEM((D, 256), BF16),
            pltpu.VMEM((D, 256), BF16),
            pltpu.VMEM((D, 512), BF16),
            pltpu.VMEM((2 * HALF, D), BF16),
            pltpu.VMEM((4, 2, HALF, 256), BF16),
            pltpu.VMEM((4, 2, HALF, 128), BF16),
            pltpu.VMEM((NZ, NX * 2 * HALF, 256), BF16),
            pltpu.VMEM((NZ, HALF, 128), BF16),
            pltpu.VMEM((NZ, 2 * HALF, 128), BF16),
            pltpu.VMEM((2 * HALF + 32, 512), F32),
            pltpu.VMEM((32, 512), BF16),
            pltpu.VMEM((32, 512), BF16),
            pltpu.VMEM((2 * HALF, 512), F32),
            pltpu.VMEM((2 * HALF, 128), F32),
            pltpu.VMEM((2 * HALF, 128), F32),
            pltpu.VMEM((2, HALF, 512), BF16),
            pltpu.VMEM((HALF, 512), BF16),
            pltpu.VMEM((NZ, 8, 256), F32),
            pltpu.VMEM((NZ, 144, 256), F32),
            pltpu.VMEM((1024, 256), F32),
            pltpu.VMEM((1024, 256), F32),
            pltpu.VMEM((8, 256), F32),
            pltpu.VMEM((8, 256), F32),
            pltpu.VMEM((2, 16, 8, 256), F32),
            pltpu.VMEM((128, 128), F32),
            pltpu.VMEM((NZ, HALF, 128), BF16),
            pltpu.VMEM((NZ, HALF, 128), BF16),
            pltpu.VMEM((NZ, 8, 128), F32),
            pltpu.VMEM((4, 2, 8, 128), F32),
            pltpu.VMEM((8, 128), F32),
            pltpu.VMEM((8, 128), F32),
            pltpu.VMEM((NY, 2, 2, 512, 512), BF16),
            pltpu.VMEM((HALF, D), F32),
            dma((7,)),
            dma((2,)),
            dma((8,)),
            dma((8,)),
            dma((NZ,)),
            dma((NZ,)),
            dma((4, NZ)),
            dma((4, NZ)),
            dma((4, NZ)),
            dma((4, NZ)),
            dma((2,)),
            dma((2,)),
            dma((2,)),
            dma((2,)),
            dma((NZ,)),
            dma((NZ,)),
            dma((NZ,)),
            dma((4, 2)),
            dma((3, 2)),
            dma((3, 2)),
            dma((3, 2)),
            dma((3, 2)),
            dma((3, 2)),
            dma((3, 2)),
            dma((4, 2)),
            dma((4, 2)),
            dma((2,)),
        ],
        compiler_params=pltpu.CompilerParams(
            collective_id=0, has_side_effects=True, vmem_limit_bytes=60 * 1024 * 1024
        ),
        name="mixer",
    )(
        inputs[0],
        norm_gain[None],
        conv_kernel,
        conv_gain[None],
        head_gain[None],
        lambda_head,
        w_glu_value,
        w_glu_gate,
        w_query_one,
        w_query_two,
        w_key_one,
        w_key_two,
        w_value,
        w_out_conv,
        w_out_attn,
    )
    return (mixed[None], logs[None])


def solution(mesh):
    return jax.shard_map(
        body,
        mesh=mesh,
        in_specs=(
            P("fs", ("sp", "tp"), None),
            P(),
            P(None, "tp"),
            P(None, "tp"),
            P(None, "tp"),
            P(None, "tp"),
            P(None, "tp"),
            P(None, "tp"),
            P(None, "tp"),
            P(None, "tp"),
            P("tp"),
            P(),
            P("tp"),
            P("tp", "fs"),
            P("tp", "fs"),
        ),
        out_specs=(P("fs", ("sp", "tp"), None), P("fs", None, "tp", "sp")),
        check_vma=False,
    )
```

```python
import jax
import jax.numpy as jnp
from jax import lax
from jax.experimental import pallas as pl
from jax.experimental.pallas import tpu as pltpu
from jax.sharding import PartitionSpec as P

D = 2048
DC = 1024
HD = 64
CW = 31
NZ = 8
NX = 4
NY = 4
HALF = 128
Z_GATE = 2
V_SPLIT = 5
W_THREE = 5
NEG_FILL = -1e30
EPSILON = 1e-05
HEAD_SCALE = 0.8
MESH = pl.DeviceIdType.MESH
F32 = jnp.float32
BF16 = jnp.bfloat16


def remote(src, dst, send_sem, recv_sem, device):
    return pltpu.make_async_remote_copy(
        src_ref=src,
        dst_ref=dst,
        send_sem=send_sem,
        recv_sem=recv_sem,
        device_id=device,
        device_id_type=MESH,
    )


def kernel(
    x_ref,
    gain_ref,
    ck_ref,
    cg_ref,
    hg_ref,
    lam_ref,
    wgv_hbm,
    wgg_hbm,
    wq1_hbm,
    wq2_hbm,
    wk1_hbm,
    wk2_hbm,
    wv_hbm,
    woc_hbm,
    woa_hbm,
    out_ref,
    log_ref,
    wgv,
    wgg,
    wq1,
    wq2,
    wk1,
    wk2,
    wv,
    normed,
    k_send,
    v_send,
    q_send,
    k_buf,
    v_buf,
    q_raw,
    qs,
    gated_ext,
    halo_send,
    halo_recv,
    convd,
    sums_send,
    sums_recv,
    conv_full,
    conv_send,
    m_buf,
    acc,
    score_a,
    score_b,
    max_a,
    max_b,
    bias,
    gain_t,
    ret_send,
    attn_buf,
    lsend,
    log_buf,
    lam_own,
    lam_recv,
    w_buf,
    acc_out,
    load_sem,
    norm_sem,
    z_ss,
    z_rs,
    xs_ss,
    xs_rs,
    d_ss,
    d_rs,
    halo_sem,
    sums_sem,
    cx_sem,
    lam_sem,
    ret_ss,
    ret_rs,
    log_ss,
    log_rs,
    w_ss,
    w_rs,
    wx_ss,
    wx_rs,
    wd_ss,
    wd_rs,
    wp_ss,
    wp_rs,
    own_sem,
):
    me = lax.axis_index("sp")
    y = lax.axis_index("fs")
    c = lax.axis_index("tp")
    z, x = me // NX, me % NX
    other = 1 - c
    xr, xl, xo = (x + 1) % NX, (x + 3) % NX, (x + 2) % NX
    yr, yl, yo = (y + 1) % NY, (y + 3) % NY, (y + 2) % NY
    src_tp = z // 4
    own_head = z % 4
    local = src_tp == c
    partner = {"tp": other}
    right = {"sp": z * NX + xr}
    left = {"sp": z * NX + xl}
    up = {"fs": yr}
    down = {"fs": yl}
    following = {"sp": (me + 1) % (NZ * NX)}
    preceding = {"sp": (me + NZ * NX - 1) % (NZ * NX)}
    pending = []

    def begin(copy):
        copy.start()
        pending.append(copy)
        return copy

    loads = []
    for index, (src, dst) in enumerate(
        ((wk1_hbm, wk1), (wk2_hbm, wk2), (wv_hbm, wv), (wq1_hbm, wq1), (wq2_hbm, wq2),
         (wgv_hbm, wgv), (wgg_hbm, wgg))
    ):
        loads.append(pltpu.make_async_copy(src, dst, load_sem.at[index]))
        if index < 2:
            loads[-1].start()

    barrier = pltpu.get_barrier_semaphore()
    for device in (partner, right, left, up, down, following, preceding):
        pl.semaphore_signal(barrier, inc=1, device_id=device, device_id_type=MESH)
    for step in range(1, NZ):
        for core in range(2):
            pl.semaphore_signal(
                barrier,
                inc=1,
                device_id={"sp": ((z + step) % NZ) * NX + x, "tp": core},
                device_id_type=MESH,
            )

    my_rows = pl.multiple_of(c * HALF, HALF)
    peer_rows = pl.multiple_of(other * HALF, HALF)
    for part in range(4):
        rows_f = x_ref[part * 32 : part * 32 + 32, :].astype(F32)
        scale = lax.rsqrt(jnp.mean(rows_f * rows_f, axis=-1, keepdims=True) + EPSILON)
        normed[pl.ds(my_rows + part * 32, 32), :] = (rows_f * scale * gain_ref[...]).astype(BF16)

    lane = lax.broadcasted_iota(jnp.int32, (HALF, 128), 1)
    low = lane < HD

    def head_pair(one, two, head):
        pair = slice((head // 2) * 128, (head // 2) * 128 + 128)
        first, second = one[:, pair], two[:, pair]
        if head % 2 == 0:
            return jnp.where(low, first, pltpu.roll(second, HD, 1))
        return jnp.where(low, pltpu.roll(first, HD, 1), second)

    def project(rows, index, weight, fresh):
        if fresh:
            loads[index].wait()
        return jnp.dot(normed[pl.ds(rows, HALF), :], weight[...], preferred_element_type=F32)

    def project_keys(rows, half, fresh):
        one = project(rows, 0, wk1, fresh)
        two = project(rows, 1, wk2, fresh)
        for head in range(4):
            k_send[head, half] = head_pair(one, two, head).astype(BF16)

    def project_values(rows, half, fresh):
        values = project(rows, 2, wv, fresh)
        for head in range(4):
            v_send[head, half] = jnp.transpose(values[:, head * 128 : head * 128 + 128]).astype(BF16)

    def project_queries(rows, half, fresh):
        one = project(rows, 3, wq1, fresh)
        two = project(rows, 4, wq2, fresh)
        for head in range(4):
            q_send[head, half] = (head_pair(one, two, head) * (HD**-0.5)).astype(BF16)

    def project_glu(rows, fresh):
        block = normed[pl.ds(rows, HALF), :]
        if fresh:
            loads[5].wait()
            loads[6].wait()
        value = jnp.dot(block, wgv[...], preferred_element_type=F32).astype(BF16).astype(F32)
        gate = jnp.dot(block, wgg[...], preferred_element_type=F32).astype(BF16).astype(F32)
        gated = (value * jax.nn.sigmoid(gate)).astype(BF16)
        gated_ext[pl.ds(pl.multiple_of(rows + 32, 32), HALF), :] = gated.astype(F32)

    project_keys(my_rows, c, True)
    for load in loads[2:]:
        load.start()
    for index in range(4):
        lam_own[index : index + 1, :] = jnp.full((1, 128), lam_ref[index], F32)
    lam_own[4:8, :] = jnp.zeros((4, 128), F32)

    pl.semaphore_wait(barrier, 7 + 2 * (NZ - 1))

    mine = normed.at[pl.ds(my_rows, HALF), :]
    norm_copy = begin(remote(mine, mine, norm_sem.at[0], norm_sem.at[1], partner))

    blocks = (k_buf, v_buf)

    def slot(kind, zs, xs, cs):
        return blocks[kind].at[zs, pl.ds(pl.multiple_of((xs * 2 + cs) * HALF, HALF), HALF), :]

    def slot_half(kind, zs, xs, cs, part):
        start = pl.multiple_of((xs * 2 + cs) * HALF + part * (HALF // 2), HALF // 2)
        return blocks[kind].at[zs, pl.ds(start, HALF // 2), :]

    u = z % 4
    ranks = (u, u + 1 - 2 * (u % 2), 2 - u // 2, 3 * (1 - u // 2))
    same = 1 - src_tp - c + 2 * src_tp * c
    z_sends = []

    sources = (k_send, v_send, q_send)

    def z_send(kind, half, base):
        for rank in range(4):
            head = same * ranks[rank] + (1 - same) * ranks[3 - rank]
            target = 4 * c + head
            landing = q_raw.at[z] if kind == 2 else slot(kind, z, x, half)
            copy = remote(
                sources[kind].at[head, half],
                landing,
                z_ss.at[kind, base + rank],
                z_rs.at[kind, z],
                {"sp": target * NX + x, "tp": half},
            )
            away = jnp.logical_not((target == z) & (half == c))
            z_sends.append((away, copy))

            @pl.when(away)
            def _(copy=copy):
                copy.start()

    z_send(0, c, 0)
    project_values(my_rows, c, True)

    @pl.when(local)
    def _():
        mine = pl.ds(pl.multiple_of((x * 2 + c) * HALF, HALF), HALF)
        k_buf[z, mine, :] = k_send[own_head, c]
        v_buf[z, mine, :] = v_send[own_head, c]

    w_hbm = (woc_hbm, woa_hbm)

    def w_own(side, kind, device):
        begin(remote(w_hbm[kind], w_buf.at[y, c, kind], w_ss.at[side, kind], w_rs.at[side, kind], device))

    w_own(0, 0, up)
    w_own(1, 1, down)
    lam_copy = begin(remote(lam_own, lam_recv, lam_sem.at[0], lam_sem.at[1], partner))

    project_glu(my_rows, True)
    norm_copy.wait_recv()
    project_keys(peer_rows, other, False)
    z_send(0, other, 4)
    project_glu(peer_rows, False)
    halo_send[...] = gated_ext[2 * HALF :, :].astype(BF16)
    halo_copy = begin(remote(halo_send, halo_recv, halo_sem.at[0], halo_sem.at[1], following))
    project_values(peer_rows, other, False)
    project_queries(my_rows, c, True)
    project_queries(peer_rows, other, False)

    @pl.when(local)
    def _():
        q_raw[z] = q_send[own_head, c]

    own_w = []
    for kind in range(2):
        own = pltpu.make_async_copy(w_hbm[kind], w_buf.at[y, c, kind], own_sem.at[kind])
        own.start()
        own_w.append(own)
        begin(remote(w_hbm[kind], w_buf.at[y, c, kind], wd_ss.at[0, kind], wd_rs.at[0, kind], partner))

    taps = ck_ref[...].astype(F32)

    def conv_chunk(part):
        base = part * 32
        total = None
        for shift in range(8):
            partial = None
            span = 32 if shift == 0 else 40
            for group in range(5):
                tap = 8 * group + shift - 2
                if tap < 0 or tap >= CW:
                    continue
                term = taps[tap : tap + 1, :] * gated_ext[base + 8 * group : base + 8 * group + span, :]
                partial = term if partial is None else partial + term
            moved = partial[shift : shift + 32, :]
            total = moved if total is None else total + moved
        convd[base : base + 32, :] = total
        sums = jnp.sum(total, axis=-1, keepdims=True)
        squares = jnp.sum(total * total, axis=-1, keepdims=True)
        sums_send[base : base + 32, :] = jnp.where(low[:32], sums, squares)

    def z_wait(kind, zs):
        ref = q_raw.at[zs] if kind == 2 else slot(kind, zs, x, c)

        @pl.when(jnp.logical_not((zs == z) & local))
        def _():
            remote(ref, ref, z_ss.at[kind, 0], z_rs.at[kind, zs], partner).wait_recv()

    def pass_on(kind, ref, arrival, device):
        remote(ref, ref, xs_ss.at[kind], arrival, device).start()

    def share(kind, ref, zs):
        remote(ref, ref, d_ss.at[kind], d_rs.at[kind, zs], partner).start()

    def arrive(kind, rows, arrival):
        ref = blocks[kind].at[0, pl.ds(0, rows), :]
        remote(ref, ref, xs_ss.at[kind], arrival, partner).wait_recv()

    def stage_one(kind, zs):
        ref = slot(kind, zs, x, c)
        pass_on(kind, ref, xs_rs.at[kind, 0, zs], right)
        pass_on(kind, ref, xs_rs.at[kind, 0, zs], left)
        share(kind, ref, zs)

    def stage_queries(zs):
        z_wait(2, zs)
        rows = q_raw[zs]
        zero = jnp.zeros_like(rows)
        qs[zs, :HALF] = jnp.where(low, rows, zero)
        qs[zs, HALF:] = jnp.where(low, zero, rows)

    def stage_two(kind, zs):
        arrive(kind, 2 * HALF, xs_rs.at[kind, 0, zs])
        pass_on(kind, slot_half(kind, zs, xl, c, 0), xs_rs.at[kind, 1, zs], right)
        pass_on(kind, slot_half(kind, zs, xr, c, 1), xs_rs.at[kind, 1, zs], left)
        share(kind, slot(kind, zs, xl, c), zs)
        share(kind, slot(kind, zs, xr, c), zs)

    def stage_three(kind, zs):
        arrive(kind, HALF, xs_rs.at[kind, 1, zs])
        share(kind, slot(kind, zs, xo, c), zs)

    def stage_four(kind, zs):
        arrive(kind, 4 * HALF, d_rs.at[kind, zs])

    def sent_all(kind):
        ref = blocks[kind].at[pl.ds(0, 3)]
        remote(ref, ref, xs_ss.at[kind], d_rs.at[0, 0], partner).wait_send()
        ref = blocks[kind].at[pl.ds(0, 4)]
        remote(ref, ref, d_ss.at[kind], d_rs.at[0, 0], partner).wait_send()

    def w_wait(source, kind, side):
        ref = w_buf.at[source, c, kind]
        remote(ref, ref, w_ss.at[side, kind], w_rs.at[side, kind], up).wait_recv()

    def w_share(source, kind, relation):
        ref = w_buf.at[source, c, kind]
        begin(remote(ref, ref, wd_ss.at[relation, kind], wd_rs.at[relation, kind], partner))

    def piece(source, core, kind, xs):
        return w_buf.at[source, core, kind, pl.ds(pl.multiple_of(xs * 128, 128), 128), :]

    def piece_share(kind, relation, xs):
        ref = piece(yo, c, kind, xs)
        begin(remote(ref, ref, wp_ss.at[relation, kind], wp_rs.at[relation, kind], partner))

    def w_one():
        w_wait(yl, 0, 0)
        ref = piece(yl, c, 0, x)
        begin(remote(ref, ref, w_ss.at[2, 0], w_rs.at[2, 0], up))
        w_own(0, 1, up)
        w_wait(yr, 1, 1)
        ref = piece(yr, c, 1, x)
        begin(remote(ref, ref, w_ss.at[2, 1], w_rs.at[2, 1], down))
        w_own(1, 0, down)
        w_share(yl, 0, 1)
        w_share(yr, 1, 2)

    def w_two():
        for kind in range(2):
            ref = piece(yo, c, kind, x)
            remote(ref, ref, w_ss.at[2, kind], w_rs.at[2, kind], up).wait_recv()
            begin(remote(ref, ref, wx_ss.at[0, kind], wx_rs.at[0, kind], right))
            begin(remote(ref, ref, wx_ss.at[1, kind], wx_rs.at[1, kind], left))
            piece_share(kind, 0, x)

    def w_three():
        for kind in range(2):
            for side, xs in ((0, xl), (1, xr)):
                ref = piece(yo, c, kind, xs)
                remote(ref, ref, wx_ss.at[side, kind], wx_rs.at[side, kind], right).wait_recv()
                if side == kind:
                    device = right if side == 0 else left
                    begin(remote(ref, ref, wx_ss.at[2, kind], wx_rs.at[2, kind], device))
                piece_share(kind, 1 + side, xs)

    def w_four():
        w_wait(yl, 1, 0)
        w_share(yl, 1, 1)
        w_wait(yr, 0, 1)
        w_share(yr, 0, 2)
        for kind in range(2):
            ref = piece(yo, c, kind, xo)
            remote(ref, ref, wx_ss.at[2, kind], wx_rs.at[2, kind], right).wait_recv()
            piece_share(kind, 3, xo)

    def w_five(kind):
        for relation, source in enumerate((y, yl, yr)):
            ref = w_buf.at[source, other, kind]
            remote(ref, ref, wd_ss.at[relation, kind], wd_rs.at[relation, kind], partner).wait_recv()
        for relation, xs in enumerate((x, xl, xr, xo)):
            ref = piece(yo, other, kind, xs)
            remote(ref, ref, wp_ss.at[relation, kind], wp_rs.at[relation, kind], partner).wait_recv()

    def conv_finish():
        sums_copy.wait_recv()
        for half in range(2):
            rows = slice(half * HALF, half * HALF + HALF)
            row_sums = sums_send[rows, :] + sums_recv[rows, :]
            mean = row_sums[:, 0:1] * (1.0 / DC)
            square = row_sums[:, HD : HD + 1] * (1.0 / DC)
            scaled = (convd[rows, :] - mean) * lax.rsqrt(square - mean * mean + EPSILON) * cg_ref[...]
            result = (scaled * jax.nn.sigmoid(scaled)).astype(BF16)

            @pl.when(c == half)
            def _(result=result):
                conv_full[c] = result

            @pl.when(c != half)
            def _(result=result):
                conv_send[...] = result

        return begin(remote(conv_send, conv_full.at[c], cx_sem.at[0], cx_sem.at[1], partner))

    m_buf[...] = jnp.full_like(m_buf, NEG_FILL)
    acc[...] = jnp.zeros_like(acc)
    bias[0] = jnp.zeros((16, 8, 256), F32)
    query_segment = (x * 4 + c * 2) + (
        (lax.broadcasted_iota(jnp.int32, (8, 256), 1) & (HALF - 1)) >> 6
    )
    for segment in range(16):
        bias[1, segment] = jnp.where(query_segment >= segment, 0.0, NEG_FILL)
    gain_t[...] = jnp.transpose(jnp.broadcast_to(hg_ref[...], (128, 128))) * HEAD_SCALE

    def place(index):
        odd = index % 2
        offset = odd * ((index + 1) // 2) + (1 - odd) * (NZ - index // 2)
        return (z + offset) % NZ

    before = (z * (z + 1)) // 2

    def which(t):
        skipped = t + jnp.where(t >= before, z + 1, 0)
        t = jnp.where(t >= 35 - z, t - 35 + z + before, skipped)
        i = 0
        for bound in (1, 3, 6, 10, 15, 21, 28):
            i = i + jnp.where(t >= bound, 1, 0)
        j = t - (i * (i + 1)) // 2
        return j, i, (j + 1) // (i + 1)

    def scores(t, score_ref, max_ref):
        s, zt, kind = which(t)
        queries = qs[zt]
        best = None
        for start in range(0, 1024, 256):
            block = lax.dot_general(
                k_buf[s, start : start + 256, :],
                queries,
                (((1,), (1,)), ((), ())),
                preferred_element_type=F32,
            )
            score_ref[start : start + 256] = block
            for inner in range(4):
                top = None
                for row in range(inner * 64, inner * 64 + 64, 8):
                    top = block[row : row + 8] if top is None else jnp.maximum(top, block[row : row + 8])
                top = top + bias[kind, start // 64 + inner]
                best = top if best is None else jnp.maximum(best, top)
        max_ref[...] = best

    ones = jnp.ones((16, 256), BF16)

    def absorb(t, score_ref, max_ref):
        s, zt, kind = which(t)
        old = m_buf[zt, 0:1]
        new = jnp.maximum(old, jnp.max(max_ref[...], axis=0, keepdims=True))
        factor = jnp.exp(old - new)
        total = None
        for start in range(0, 1024, 256):
            weights = []
            for inner in range(4):
                row = start + inner * 64
                shifted = new - bias[kind, row // 64, 0:1]
                weights.append(jnp.exp(score_ref[row : row + 64] - shifted).astype(BF16))
            lhs = jnp.concatenate(
                [
                    jnp.concatenate(
                        [
                            v_buf[s, start : start + 128, :],
                            v_buf[s, start + 128 : start + 256, :],
                        ],
                        axis=1,
                    ),
                    ones,
                ],
                axis=0,
            )
            part = jnp.dot(lhs, jnp.concatenate(weights, axis=0), preferred_element_type=F32)
            total = part if total is None else total + part
        acc[zt] = acc[zt] * factor + total
        m_buf[zt] = jnp.broadcast_to(new, (8, 256))

    def ret_copy(s):
        return remote(
            ret_send.at[s], attn_buf.at[z], ret_ss, ret_rs.at[z], {"sp": s * NX + x}
        )

    def log_copy(s):
        return remote(
            lsend.at[s], log_buf.at[own_head, c], log_ss.at[s], log_rs.at[own_head, c],
            {"sp": s * NX + x, "tp": src_tp},
        )

    def finish(s):
        sums = acc[s, 128:129, :]
        normal = acc[s, 0:128, :] * (1.0 / sums)
        lam_row = jnp.where(local, lam_own[pl.ds(own_head, 1), :], lam_recv[pl.ds(own_head, 1), :])
        head_out = normal[:, :HALF] - lam_row * normal[:, HALF:]
        head_out = (
            head_out
            * lax.rsqrt(jnp.mean(head_out * head_out, axis=0, keepdims=True) + EPSILON)
            * gain_t[...]
        )
        head_out = jnp.transpose(head_out).astype(BF16)
        logs = m_buf[s, 0:1] + jnp.log(sums)
        sub = lax.broadcasted_iota(jnp.int32, (8, 128), 0)
        log_rows = jnp.where(sub == 0, logs[:, :HALF], logs[:, HALF:])
        ret_send[s] = head_out
        lsend[s] = log_rows

        @pl.when(s == z)
        def _():
            attn_buf[z] = head_out

        @pl.when((s == z) & local)
        def _():
            log_buf[own_head, c] = log_rows

        @pl.when(s != z)
        def _():
            ret_copy(s).start()

        @pl.when(jnp.logical_not((s == z) & local))
        def _():
            log_copy(s).start()

    def finish_one_of(t):
        _, first, first_done = which(t)
        _, second, second_done = which(t + 1)

        def run(_, carry):
            finish(first * first_done + second * second_done)
            return carry

        lax.fori_loop(0, first_done + second_done, run, 0)

    def pair(p, carry):
        scores(2 * p + 1, score_b, max_b)
        absorb(2 * p, score_a, max_a)
        scores(2 * p + 2, score_a, max_a)
        absorb(2 * p + 1, score_b, max_b)
        finish_one_of(2 * p)
        return carry

    for part in (1, 2, 3, 4, 5, 6, 7):
        conv_chunk(part)
    for step in range(NZ):
        z_wait(0, place(step))
        stage_one(0, place(step))
        if step == Z_GATE:
            z_send(1, c, 0)
            z_send(1, other, 4)
    for step in range(NZ):
        stage_two(0, place(step))
    for step in range(NZ):
        z_wait(1, place(step))
        if step == Z_GATE:
            z_send(2, c, 0)
            z_send(2, other, 4)
    for step in range(V_SPLIT):
        stage_one(1, step)
    w_one()
    for step in range(NZ):
        stage_three(0, place(step))
    halo_copy.wait_recv()
    rows = halo_recv[...].astype(F32)
    gated_ext[0:32, :] = jnp.where(me == 0, jnp.zeros_like(rows), rows)
    conv_chunk(0)
    sums_copy = begin(remote(sums_send, sums_recv, sums_sem.at[0], sums_sem.at[1], partner))
    for step in range(NZ):
        stage_four(0, place(step))
    for step in range(V_SPLIT):
        stage_two(1, step)
    for step in range(V_SPLIT, NZ):
        stage_one(1, step)
    conv_copy = conv_finish()
    for step in range(V_SPLIT):
        stage_three(1, step)
    lam_copy.wait_recv()
    stage_queries(0)
    stage_four(1, 0)
    done_pairs = 0
    for index in range(NZ):
        if index + 1 < NZ:
            stage_queries(index + 1)
            stage_four(1, index + 1)
        if index == 0:
            scores(0, score_a, max_a)
        else:
            end = ((index + 1) * (index + 2) // 2 - 1) // 2
            lax.fori_loop(done_pairs, end, pair, 0)
            done_pairs = end
        if index == V_SPLIT - 3:
            for step in range(V_SPLIT, NZ):
                stage_two(1, step)
            w_two()
        if index == V_SPLIT - 2:
            for step in range(V_SPLIT, NZ):
                stage_three(1, step)
        if index == W_THREE:
            w_three()
    w_four()
    scores(35, score_b, max_b)
    absorb(34, score_a, max_a)
    absorb(35, score_b, max_b)

    def run_last(_, carry):
        finish(NZ - 1)
        return carry

    lax.fori_loop(0, (7 - z) // 7, run_last, 0)

    finish(z)

    for kind in range(2):
        own_w[kind].wait()
    conv_copy.wait_recv()
    w_five(0)
    for quarter in range(NY):
        cols = slice(quarter * 512, quarter * 512 + 512)
        acc_out[:, cols] = jnp.dot(
            conv_full[0], w_buf[quarter, 0, 0], preferred_element_type=F32
        ) + jnp.dot(conv_full[1], w_buf[quarter, 1, 0], preferred_element_type=F32)
    w_five(1)

    for hs in range(NZ):

        @pl.when(hs != z)
        def _(hs=hs):
            remote(
                attn_buf.at[hs], attn_buf.at[hs], ret_ss, ret_rs.at[hs], partner
            ).wait_recv()

    sides = [jnp.concatenate([attn_buf[4 * side + k] for k in range(4)], axis=1) for side in range(2)]
    for quarter in range(NY):
        cols = slice(quarter * 512, quarter * 512 + 512)
        result = acc_out[:, cols]
        for side in range(2):
            result = result + jnp.dot(
                sides[side], w_buf[quarter, side, 1], preferred_element_type=F32
            )
        out_ref[:, cols] = result.astype(BF16)

    for head in range(4):
        for half in range(2):
            from_self = (4 * c + head == z) & (c == half)

            @pl.when(jnp.logical_not(from_self))
            def _(head=head, half=half):
                ref = log_buf.at[head, half]
                remote(ref, ref, log_ss.at[0], log_rs.at[head, half], partner).wait_recv()

            for which_map in range(2):
                log_ref[which_map, head : head + 1, half * HALF : half * HALF + HALF] = log_buf[
                    head, half, which_map : which_map + 1, :
                ]

    for away, copy in z_sends:

        @pl.when(away)
        def _(copy=copy):
            copy.wait_send()

    for copy in pending:
        copy.wait_send()
    sent_all(0)
    sent_all(1)
    ref = ret_send.at[pl.ds(0, NZ - 1)]
    remote(ref, ref, ret_ss, ret_rs.at[0], partner).wait_send()
    for s in range(NZ):

        @pl.when(jnp.logical_not((s == z) & local))
        def _(s=s):
            log_copy(s).wait_send()


def hand_over(mixed_ref, logs_ref, mixed_out, logs_out):
    mixed_out[...] = mixed_ref[...]
    logs_out[...] = logs_ref[...]


def body(
    inputs,
    norm_gain,
    w_glu_value,
    w_glu_gate,
    w_query_one,
    w_query_two,
    w_key_one,
    w_key_two,
    w_value,
    conv_kernel,
    conv_gain,
    head_gain,
    lambda_head,
    w_out_conv,
    w_out_attn,
):
    vmem = pl.BlockSpec(memory_space=pltpu.VMEM)
    hbm = pl.BlockSpec(memory_space=pl.ANY)
    dma = pltpu.SemaphoreType.DMA
    mixed, logs = pl.pallas_call(
        kernel,
        out_shape=(
            jax.ShapeDtypeStruct((HALF, D), BF16),
            jax.ShapeDtypeStruct((2, 4, 2 * HALF), F32),
        ),
        in_specs=[vmem] * 5 + [pl.BlockSpec(memory_space=pltpu.SMEM)] + [hbm] * 9,
        out_specs=(vmem, vmem),
        scratch_shapes=[
            pltpu.VMEM((D, 512), BF16),
            pltpu.VMEM((D, 512), BF16),
            pltpu.VMEM((D, 256), BF16),
            pltpu.VMEM((D, 256), BF16),
            pltpu.VMEM((D, 256), BF16),
            pltpu.VMEM((D, 256), BF16),
            pltpu.VMEM((D, 512), BF16),
            pltpu.VMEM((2 * HALF, D), BF16),
            pltpu.VMEM((4, 2, HALF, 128), BF16),
            pltpu.VMEM((4, 2, HALF, 128), BF16),
            pltpu.VMEM((4, 2, HALF, 128), BF16),
            pltpu.VMEM((NZ, NX * 2 * HALF, 128), BF16),
            pltpu.VMEM((NZ, NX * 2 * HALF, 128), BF16),
            pltpu.VMEM((NZ, HALF, 128), BF16),
            pltpu.VMEM((NZ, 2 * HALF, 128), BF16),
            pltpu.VMEM((2 * HALF + 32, 512), F32),
            pltpu.VMEM((32, 512), BF16),
            pltpu.VMEM((32, 512), BF16),
            pltpu.VMEM((2 * HALF, 512), F32),
            pltpu.VMEM((2 * HALF, 128), F32),
            pltpu.VMEM((2 * HALF, 128), F32),
            pltpu.VMEM((2, HALF, 512), BF16),
            pltpu.VMEM((HALF, 512), BF16),
            pltpu.VMEM((NZ, 8, 256), F32),
            pltpu.VMEM((NZ, 144, 256), F32),
            pltpu.VMEM((1024, 256), F32),
            pltpu.VMEM((1024, 256), F32),
            pltpu.VMEM((8, 256), F32),
            pltpu.VMEM((8, 256), F32),
            pltpu.VMEM((2, 16, 8, 256), F32),
            pltpu.VMEM((128, 128), F32),
            pltpu.VMEM((NZ, HALF, 128), BF16),
            pltpu.VMEM((NZ, HALF, 128), BF16),
            pltpu.VMEM((NZ, 8, 128), F32),
            pltpu.VMEM((4, 2, 8, 128), F32),
            pltpu.VMEM((8, 128), F32),
            pltpu.VMEM((8, 128), F32),
            pltpu.VMEM((NY, 2, 2, 512, 512), BF16),
            pltpu.VMEM((HALF, D), F32),
            dma((7,)),
            dma((2,)),
            dma((3, 8)),
            dma((3, NZ)),
            dma((2,)),
            dma((2, 2, NZ)),
            dma((2,)),
            dma((2, NZ)),
            dma((2,)),
            dma((2,)),
            dma((2,)),
            dma((2,)),
            dma,
            dma((NZ,)),
            dma((NZ,)),
            dma((4, 2)),
            dma((3, 2)),
            dma((3, 2)),
            dma((3, 2)),
            dma((3, 2)),
            dma((3, 2)),
            dma((3, 2)),
            dma((4, 2)),
            dma((4, 2)),
            dma((2,)),
        ],
        compiler_params=pltpu.CompilerParams(
            collective_id=0, has_side_effects=True, vmem_limit_bytes=60 * 1024 * 1024
        ),
        name="mixer",
    )(
        inputs[0],
        norm_gain[None],
        conv_kernel,
        conv_gain[None],
        head_gain[None],
        lambda_head,
        w_glu_value,
        w_glu_gate,
        w_query_one,
        w_query_two,
        w_key_one,
        w_key_two,
        w_value,
        w_out_conv,
        w_out_attn,
    )
    mixed, logs = pl.pallas_call(
        hand_over,
        out_shape=(
            jax.ShapeDtypeStruct((HALF, D), BF16),
            jax.ShapeDtypeStruct((2, 4, 2 * HALF), F32),
        ),
        in_specs=[vmem, vmem],
        out_specs=(vmem, vmem),
        name="hand_over",
    )(mixed, logs)
    return (mixed[None], logs[None])


def solution(mesh):
    return jax.shard_map(
        body,
        mesh=mesh,
        in_specs=(
            P("fs", ("sp", "tp"), None),
            P(),
            P(None, "tp"),
            P(None, "tp"),
            P(None, "tp"),
            P(None, "tp"),
            P(None, "tp"),
            P(None, "tp"),
            P(None, "tp"),
            P(None, "tp"),
            P("tp"),
            P(),
            P("tp"),
            P("tp", "fs"),
            P("tp", "fs"),
        ),
        out_specs=(P("fs", ("sp", "tp"), None), P("fs", None, "tp", "sp")),
        check_vma=False,
    )
```

```python
import jax
import jax.numpy as jnp
from jax import lax
from jax.experimental import pallas as pl
from jax.experimental.pallas import tpu as pltpu
from jax.sharding import PartitionSpec as P

D = 2048
DC = 1024
HD = 64
CW = 31
NZ = 8
NX = 4
NY = 4
HALF = 128
Z_GATE = 0
Q_GATE = 4
FAR_FIRST = (0, 4, 5, 3, 6, 2, 7, 1)
V_SPLIT = 4
W_THREE = 5
NEG_FILL = -1e30
EPSILON = 1e-05
HEAD_SCALE = 0.8
MESH = pl.DeviceIdType.MESH
F32 = jnp.float32
BF16 = jnp.bfloat16


def remote(src, dst, send_sem, recv_sem, device):
    return pltpu.make_async_remote_copy(
        src_ref=src,
        dst_ref=dst,
        send_sem=send_sem,
        recv_sem=recv_sem,
        device_id=device,
        device_id_type=MESH,
    )


def kernel(
    x_ref,
    gain_ref,
    ck_ref,
    cg_ref,
    hg_ref,
    lam_ref,
    wgv_hbm,
    wgg_hbm,
    wq1_hbm,
    wq2_hbm,
    wk1_hbm,
    wk2_hbm,
    wv_hbm,
    woc_hbm,
    woa_hbm,
    out_ref,
    log_ref,
    wgv,
    wgg,
    wq1,
    wq2,
    wk1,
    wk2,
    wv,
    normed,
    k_send,
    v_send,
    q_send,
    k_buf,
    v_buf,
    q_raw,
    qs,
    gated_ext,
    halo_send,
    halo_recv,
    convd,
    sums_send,
    sums_recv,
    conv_full,
    conv_send,
    m_buf,
    acc,
    score_a,
    score_b,
    max_a,
    max_b,
    bias,
    gain_t,
    ret_send,
    attn_buf,
    lsend,
    log_buf,
    lam_own,
    lam_recv,
    w_buf,
    acc_out,
    load_sem,
    norm_sem,
    z_ss,
    z_rs,
    xs_ss,
    xs_rs,
    d_ss,
    d_rs,
    halo_sem,
    sums_sem,
    cx_sem,
    lam_sem,
    ret_ss,
    ret_rs,
    log_ss,
    log_rs,
    w_ss,
    w_rs,
    wx_rs,
    wd_rs,
    own_sem,
):
    me = lax.axis_index("sp")
    y = lax.axis_index("fs")
    c = lax.axis_index("tp")
    z, x = me // NX, me % NX
    other = 1 - c
    xr, xl, xo = (x + 1) % NX, (x + 3) % NX, (x + 2) % NX
    yr, yl, yo = (y + 1) % NY, (y + 3) % NY, (y + 2) % NY
    src_tp = z // 4
    own_head = z % 4
    local = src_tp == c
    partner = {"tp": other}
    right = {"sp": z * NX + xr}
    left = {"sp": z * NX + xl}
    up = {"fs": yr}
    down = {"fs": yl}
    following = {"sp": (me + 1) % (NZ * NX)}
    preceding = {"sp": (me + NZ * NX - 1) % (NZ * NX)}
    pending = []

    def begin(copy):
        copy.start()
        pending.append(copy)
        return copy

    loads = []
    for index, (src, dst) in enumerate(
        ((wk1_hbm, wk1), (wk2_hbm, wk2), (wv_hbm, wv), (wq1_hbm, wq1), (wq2_hbm, wq2),
         (wgv_hbm, wgv), (wgg_hbm, wgg))
    ):
        loads.append(pltpu.make_async_copy(src, dst, load_sem.at[index]))
        if index < 2:
            loads[-1].start()

    barrier = pltpu.get_barrier_semaphore()
    for device in (partner, right, left, up, down, following, preceding):
        pl.semaphore_signal(barrier, inc=1, device_id=device, device_id_type=MESH)
    for step in range(1, NZ):
        for core in range(2):
            pl.semaphore_signal(
                barrier,
                inc=1,
                device_id={"sp": ((z + step) % NZ) * NX + x, "tp": core},
                device_id_type=MESH,
            )

    my_rows = pl.multiple_of(c * HALF, HALF)
    peer_rows = pl.multiple_of(other * HALF, HALF)
    for part in range(4):
        rows_f = x_ref[part * 32 : part * 32 + 32, :].astype(F32)
        scale = lax.rsqrt(jnp.mean(rows_f * rows_f, axis=-1, keepdims=True) + EPSILON)
        normed[pl.ds(my_rows + part * 32, 32), :] = (rows_f * scale * gain_ref[...]).astype(BF16)

    lane = lax.broadcasted_iota(jnp.int32, (HALF, 128), 1)
    low = lane < HD

    def head_pair(one, two, head):
        pair = slice((head // 2) * 128, (head // 2) * 128 + 128)
        first, second = one[:, pair], two[:, pair]
        if head % 2 == 0:
            return jnp.where(low, first, pltpu.roll(second, HD, 1))
        return jnp.where(low, pltpu.roll(first, HD, 1), second)

    def project(rows, index, weight, fresh):
        if fresh:
            loads[index].wait()
        return jnp.dot(normed[pl.ds(rows, HALF), :], weight[...], preferred_element_type=F32)

    def project_keys(rows, half, fresh):
        one = project(rows, 0, wk1, fresh)
        two = project(rows, 1, wk2, fresh)
        for head in range(4):
            k_send[head, half] = head_pair(one, two, head).astype(BF16)

    def project_values(rows, half, fresh):
        values = project(rows, 2, wv, fresh)
        for head in range(4):
            v_send[head, half] = jnp.transpose(values[:, head * 128 : head * 128 + 128]).astype(BF16)

    def project_queries(rows, half, fresh):
        one = project(rows, 3, wq1, fresh)
        two = project(rows, 4, wq2, fresh)
        for head in range(4):
            q_send[head, half] = (head_pair(one, two, head) * (HD**-0.5)).astype(BF16)

    def project_glu(rows, fresh):
        block = normed[pl.ds(rows, HALF), :]
        if fresh:
            loads[5].wait()
            loads[6].wait()
        value = jnp.dot(block, wgv[...], preferred_element_type=F32).astype(BF16).astype(F32)
        gate = jnp.dot(block, wgg[...], preferred_element_type=F32).astype(BF16).astype(F32)
        gated = (value * jax.nn.sigmoid(gate)).astype(BF16)
        gated_ext[pl.ds(pl.multiple_of(rows + 32, 32), HALF), :] = gated.astype(F32)

    project_keys(my_rows, c, True)
    for load in loads[2:]:
        load.start()
    for index in range(4):
        lam_own[index : index + 1, :] = jnp.full((1, 128), lam_ref[index], F32)
    lam_own[4:8, :] = jnp.zeros((4, 128), F32)

    pl.semaphore_wait(barrier, 7 + 2 * (NZ - 1))

    mine = normed.at[pl.ds(my_rows, HALF), :]
    norm_copy = begin(remote(mine, mine, norm_sem.at[0], norm_sem.at[1], partner))

    blocks = (k_buf, v_buf)

    def slot(kind, zs, xs, cs):
        return blocks[kind].at[zs, pl.ds(pl.multiple_of((xs * 2 + cs) * HALF, HALF), HALF), :]

    def slot_half(kind, zs, xs, cs, part):
        start = pl.multiple_of((xs * 2 + cs) * HALF + part * (HALF // 2), HALF // 2)
        return blocks[kind].at[zs, pl.ds(start, HALF // 2), :]

    u = z % 4
    ranks = (u, u + 1 - 2 * (u % 2), 2 - u // 2, 3 * (1 - u // 2))
    same = 1 - src_tp - c + 2 * src_tp * c

    sources = (k_send, v_send, q_send)

    def z_send(kind, half):
        for rank in (3, 2, 1, 0):
            head = same * ranks[rank] + (1 - same) * ranks[3 - rank]
            target = 4 * c + head
            landing = q_raw.at[z] if kind == 2 else slot(kind, z, x, half)
            copy = remote(
                sources[kind].at[head, half],
                landing,
                z_ss.at[kind],
                z_rs.at[kind, z],
                {"sp": target * NX + x, "tp": half},
            )
            away = jnp.logical_not((target == z) & (half == c))

            @pl.when(away)
            def _(copy=copy):
                copy.start()

    z_send(0, c)
    project_values(my_rows, c, True)

    @pl.when(local)
    def _():
        mine = pl.ds(pl.multiple_of((x * 2 + c) * HALF, HALF), HALF)
        k_buf[z, mine, :] = k_send[own_head, c]
        v_buf[z, mine, :] = v_send[own_head, c]

    def z_wait(kind, zs):
        ref = q_raw.at[zs] if kind == 2 else slot(kind, zs, x, c)

        @pl.when(jnp.logical_not((zs == z) & local))
        def _():
            remote(ref, ref, z_ss.at[kind], z_rs.at[kind, zs], partner).wait_recv()

    def pass_on(kind, ref, arrival, device):
        remote(ref, ref, xs_ss.at[kind], arrival, device).start()

    def share(kind, ref, zs):
        remote(ref, ref, d_ss.at[kind], d_rs.at[kind, zs], partner).start()

    def arrive(kind, rows, arrival):
        ref = blocks[kind].at[0, pl.ds(0, rows), :]
        remote(ref, ref, xs_ss.at[kind], arrival, partner).wait_recv()

    def stage_one(kind, zs):
        ref = slot(kind, zs, x, c)
        pass_on(kind, ref, xs_rs.at[kind, 0, zs], right)
        pass_on(kind, ref, xs_rs.at[kind, 0, zs], left)
        share(kind, ref, zs)

    w_hbm = (woc_hbm, woa_hbm)

    def w_own(side, kind, device):
        remote(w_hbm[kind], w_buf.at[y, c, kind], w_ss, w_rs.at[side, kind], device).start()

    w_own(0, 0, up)
    w_own(1, 1, down)
    lam_copy = begin(remote(lam_own, lam_recv, lam_sem.at[0], lam_sem.at[1], partner))

    project_glu(my_rows, True)
    norm_copy.wait_recv()
    project_keys(peer_rows, other, False)
    z_send(0, other)
    project_glu(peer_rows, False)
    halo_send[...] = gated_ext[2 * HALF :, :].astype(BF16)
    halo_copy = begin(remote(halo_send, halo_recv, halo_sem.at[0], halo_sem.at[1], following))
    project_values(peer_rows, other, False)
    z_wait(0, z)
    stage_one(0, z)
    project_queries(my_rows, c, True)
    project_queries(peer_rows, other, False)

    @pl.when(local)
    def _():
        q_raw[z] = q_send[own_head, c]

    own_w = []
    for kind in range(2):
        own = pltpu.make_async_copy(w_hbm[kind], w_buf.at[y, c, kind], own_sem.at[kind])
        own.start()
        own_w.append(own)
        remote(w_hbm[kind], w_buf.at[y, c, kind], w_ss, wd_rs.at[kind], partner).start()

    taps = ck_ref[...].astype(F32)

    def conv_chunk(part):
        base = part * 32
        total = None
        for shift in range(8):
            partial = None
            span = 32 if shift == 0 else 40
            for group in range(5):
                tap = 8 * group + shift - 2
                if tap < 0 or tap >= CW:
                    continue
                term = taps[tap : tap + 1, :] * gated_ext[base + 8 * group : base + 8 * group + span, :]
                partial = term if partial is None else partial + term
            moved = partial[shift : shift + 32, :]
            total = moved if total is None else total + moved
        convd[base : base + 32, :] = total
        sums = jnp.sum(total, axis=-1, keepdims=True)
        squares = jnp.sum(total * total, axis=-1, keepdims=True)
        sums_send[base : base + 32, :] = jnp.where(low[:32], sums, squares)

    def stage_queries(zs):
        z_wait(2, zs)
        rows = q_raw[zs]
        zero = jnp.zeros_like(rows)
        qs[zs, :HALF] = jnp.where(low, rows, zero)
        qs[zs, HALF:] = jnp.where(low, zero, rows)

    def stage_two(kind, zs):
        arrive(kind, 2 * HALF, xs_rs.at[kind, 0, zs])
        pass_on(kind, slot_half(kind, zs, xl, c, 0), xs_rs.at[kind, 1, zs], right)
        pass_on(kind, slot_half(kind, zs, xr, c, 1), xs_rs.at[kind, 1, zs], left)
        share(kind, slot(kind, zs, xl, c), zs)
        share(kind, slot(kind, zs, xr, c), zs)

    def stage_three(kind, zs):
        arrive(kind, HALF, xs_rs.at[kind, 1, zs])
        share(kind, slot(kind, zs, xo, c), zs)

    def stage_four(kind, zs):
        arrive(kind, 4 * HALF, d_rs.at[kind, zs])

    def sent_all(kind):
        ref = blocks[kind].at[pl.ds(0, 3)]
        remote(ref, ref, xs_ss.at[kind], d_rs.at[0, 0], partner).wait_send()
        ref = blocks[kind].at[pl.ds(0, 4)]
        remote(ref, ref, d_ss.at[kind], d_rs.at[0, 0], partner).wait_send()

    def w_wait(ref, arrival):
        remote(ref, ref, w_ss, arrival, partner).wait_recv()

    def w_pass(ref, arrival, device):
        remote(ref, ref, w_ss, arrival, device).start()

    def piece(source, core, kind, xs):
        return w_buf.at[source, core, kind, pl.ds(pl.multiple_of(xs * 128, 128), 128), :]

    def w_one():
        w_wait(w_buf.at[yl, c, 0], w_rs.at[0, 0])
        w_pass(piece(yl, c, 0, x), w_rs.at[2, 0], up)
        w_own(0, 1, up)
        w_wait(w_buf.at[yr, c, 1], w_rs.at[1, 1])
        w_pass(piece(yr, c, 1, x), w_rs.at[2, 1], down)
        w_own(1, 0, down)
        w_pass(w_buf.at[yl, c, 0], wd_rs.at[0], partner)
        w_pass(w_buf.at[yr, c, 1], wd_rs.at[1], partner)

    def w_two():
        for kind in range(2):
            ref = piece(yo, c, kind, x)
            w_wait(ref, w_rs.at[2, kind])
            w_pass(ref, wx_rs.at[0, kind], right)
            w_pass(ref, wx_rs.at[1, kind], left)
            w_pass(ref, wd_rs.at[kind], partner)

    def w_three():
        for kind in range(2):
            for side, xs in ((0, xl), (1, xr)):
                ref = piece(yo, c, kind, xs)
                w_wait(ref, wx_rs.at[side, kind])
                if side == kind:
                    w_pass(ref, wx_rs.at[2, kind], right if side == 0 else left)
                w_pass(ref, wd_rs.at[kind], partner)

    def w_four():
        w_wait(w_buf.at[yr, c, 0], w_rs.at[1, 0])
        w_pass(w_buf.at[yr, c, 0], wd_rs.at[0], partner)
        w_wait(piece(yo, c, 0, xo), wx_rs.at[2, 0])
        w_pass(piece(yo, c, 0, xo), wd_rs.at[0], partner)
        w_wait(w_buf.at[yl, c, 1], w_rs.at[0, 1])
        w_pass(w_buf.at[yl, c, 1], wd_rs.at[1], partner)
        w_wait(piece(yo, c, 1, xo), wx_rs.at[2, 1])
        w_pass(piece(yo, c, 1, xo), wd_rs.at[1], partner)

    def w_five(kind):
        w_wait(w_buf.at[0], wd_rs.at[kind])

    def conv_finish():
        sums_copy.wait_recv()
        for half in range(2):
            rows = slice(half * HALF, half * HALF + HALF)
            row_sums = sums_send[rows, :] + sums_recv[rows, :]
            mean = row_sums[:, 0:1] * (1.0 / DC)
            square = row_sums[:, HD : HD + 1] * (1.0 / DC)
            scaled = (convd[rows, :] - mean) * lax.rsqrt(square - mean * mean + EPSILON) * cg_ref[...]
            result = (scaled * jax.nn.sigmoid(scaled)).astype(BF16)

            @pl.when(c == half)
            def _(result=result):
                conv_full[c] = result

            @pl.when(c != half)
            def _(result=result):
                conv_send[...] = result

        return begin(remote(conv_send, conv_full.at[c], cx_sem.at[0], cx_sem.at[1], partner))

    m_buf[...] = jnp.full_like(m_buf, NEG_FILL)
    acc[...] = jnp.zeros_like(acc)
    bias[0] = jnp.zeros((16, 8, 256), F32)
    query_segment = (x * 4 + c * 2) + (
        (lax.broadcasted_iota(jnp.int32, (8, 256), 1) & (HALF - 1)) >> 6
    )
    for segment in range(16):
        bias[1, segment] = jnp.where(query_segment >= segment, 0.0, NEG_FILL)
    gain_t[...] = jnp.transpose(jnp.broadcast_to(hg_ref[...], (128, 128))) * HEAD_SCALE

    def place(index):
        return (z + FAR_FIRST[index]) % NZ

    before = (z * (z + 1)) // 2

    def which(t):
        skipped = t + jnp.where(t >= before, z + 1, 0)
        t = jnp.where(t >= 35 - z, t - 35 + z + before, skipped)
        i = 0
        for bound in (1, 3, 6, 10, 15, 21, 28):
            i = i + jnp.where(t >= bound, 1, 0)
        j = t - (i * (i + 1)) // 2
        return j, i, (j + 1) // (i + 1)

    def scores(t, score_ref, max_ref):
        s, zt, kind = which(t)
        queries = qs[zt]
        best = None
        for start in range(0, 1024, 256):
            block = lax.dot_general(
                k_buf[s, start : start + 256, :],
                queries,
                (((1,), (1,)), ((), ())),
                preferred_element_type=F32,
            )
            score_ref[start : start + 256] = block
            for inner in range(4):
                top = None
                for row in range(inner * 64, inner * 64 + 64, 8):
                    top = block[row : row + 8] if top is None else jnp.maximum(top, block[row : row + 8])
                top = top + bias[kind, start // 64 + inner]
                best = top if best is None else jnp.maximum(best, top)
        max_ref[...] = best

    ones = jnp.ones((16, 256), BF16)

    def absorb(t, score_ref, max_ref):
        s, zt, kind = which(t)
        old = m_buf[zt, 0:1]
        new = jnp.maximum(old, jnp.max(max_ref[...], axis=0, keepdims=True))
        factor = jnp.exp(old - new)
        total = None
        for start in range(0, 1024, 256):
            weights = []
            for inner in range(4):
                row = start + inner * 64
                shifted = new - bias[kind, row // 64, 0:1]
                weights.append(jnp.exp(score_ref[row : row + 64] - shifted).astype(BF16))
            lhs = jnp.concatenate(
                [
                    jnp.concatenate(
                        [
                            v_buf[s, start : start + 128, :],
                            v_buf[s, start + 128 : start + 256, :],
                        ],
                        axis=1,
                    ),
                    ones,
                ],
                axis=0,
            )
            part = jnp.dot(lhs, jnp.concatenate(weights, axis=0), preferred_element_type=F32)
            total = part if total is None else total + part
        acc[zt] = acc[zt] * factor + total
        m_buf[zt] = jnp.broadcast_to(new, (8, 256))

    def ret_copy(s):
        return remote(
            ret_send.at[s], attn_buf.at[z], ret_ss, ret_rs, {"sp": s * NX + x}
        )

    def log_copy(s):
        return remote(
            lsend.at[s], log_buf.at[own_head, c], log_ss, log_rs,
            {"sp": s * NX + x, "tp": src_tp},
        )

    def finish(s):
        sums = acc[s, 128:129, :]
        normal = acc[s, 0:128, :] * (1.0 / sums)
        lam_row = jnp.where(local, lam_own[pl.ds(own_head, 1), :], lam_recv[pl.ds(own_head, 1), :])
        head_out = normal[:, :HALF] - lam_row * normal[:, HALF:]
        head_out = (
            head_out
            * lax.rsqrt(jnp.mean(head_out * head_out, axis=0, keepdims=True) + EPSILON)
            * gain_t[...]
        )
        head_out = jnp.transpose(head_out).astype(BF16)
        logs = m_buf[s, 0:1] + jnp.log(sums)
        sub = lax.broadcasted_iota(jnp.int32, (8, 128), 0)
        log_rows = jnp.where(sub == 0, logs[:, :HALF], logs[:, HALF:])
        ret_send[s] = head_out
        lsend[s] = log_rows

        @pl.when(s == z)
        def _():
            attn_buf[z] = head_out

        @pl.when((s == z) & local)
        def _():
            log_buf[own_head, c] = log_rows

        @pl.when(s != z)
        def _():
            ret_copy(s).start()

        @pl.when(jnp.logical_not((s == z) & local))
        def _():
            log_copy(s).start()

    def finish_one_of(t):
        _, first, first_done = which(t)
        _, second, second_done = which(t + 1)

        def run(_, carry):
            finish(first * first_done + second * second_done)
            return carry

        lax.fori_loop(0, first_done + second_done, run, 0)

    def pair(p, carry):
        scores(2 * p + 1, score_b, max_b)
        absorb(2 * p, score_a, max_a)
        scores(2 * p + 2, score_a, max_a)
        absorb(2 * p + 1, score_b, max_b)
        finish_one_of(2 * p)
        return carry

    for step in range(NZ):
        if step > 0:
            z_wait(0, place(step))
            stage_one(0, place(step))
        if step == Z_GATE:
            z_send(1, c)
            z_send(1, other)
    for step in range(NZ):
        stage_two(0, place(step))
        if step > 0:
            conv_chunk(step)
        if step == Q_GATE:
            z_send(2, c)
            z_send(2, other)
    for step in range(NZ):
        z_wait(1, place(step))
    for step in range(V_SPLIT):
        stage_one(1, step)
    w_one()
    for step in range(NZ):
        stage_three(0, place(step))
    halo_copy.wait_recv()
    rows = halo_recv[...].astype(F32)
    gated_ext[0:32, :] = jnp.where(me == 0, jnp.zeros_like(rows), rows)
    conv_chunk(0)
    sums_copy = begin(remote(sums_send, sums_recv, sums_sem.at[0], sums_sem.at[1], partner))
    for step in range(V_SPLIT):
        stage_two(1, step)
    for step in range(V_SPLIT, NZ):
        stage_one(1, step)
    conv_copy = conv_finish()
    for step in range(V_SPLIT):
        stage_three(1, step)
    lam_copy.wait_recv()
    for step in range(NZ):
        stage_four(0, place(step))
    stage_queries(0)
    stage_four(1, 0)
    done_pairs = 0
    for index in range(NZ):
        if index + 1 < NZ:
            stage_queries(index + 1)
            stage_four(1, index + 1)
        if index == 0:
            scores(0, score_a, max_a)
        else:
            end = ((index + 1) * (index + 2) // 2 - 1) // 2
            lax.fori_loop(done_pairs, end, pair, 0)
            done_pairs = end
        if index == V_SPLIT - 3:
            for step in range(V_SPLIT, NZ):
                stage_two(1, step)
        if index == V_SPLIT - 2:
            for step in range(V_SPLIT, NZ):
                stage_three(1, step)
            w_two()
        if index == W_THREE:
            w_three()
    w_four()
    scores(35, score_b, max_b)
    absorb(34, score_a, max_a)
    absorb(35, score_b, max_b)

    def run_last(_, carry):
        finish(NZ - 1)
        return carry

    lax.fori_loop(0, (7 - z) // 7, run_last, 0)

    finish(z)

    for kind in range(2):
        own_w[kind].wait()
    conv_copy.wait_recv()
    w_five(0)
    for quarter in range(NY):
        cols = slice(quarter * 512, quarter * 512 + 512)
        acc_out[:, cols] = jnp.dot(
            conv_full[0], w_buf[quarter, 0, 0], preferred_element_type=F32
        ) + jnp.dot(conv_full[1], w_buf[quarter, 1, 0], preferred_element_type=F32)
    w_five(1)

    ref = ret_send.at[pl.ds(0, NZ - 1)]
    remote(ref, ref, ret_ss, ret_rs, partner).wait_recv()

    sides = [jnp.concatenate([attn_buf[4 * side + k] for k in range(4)], axis=1) for side in range(2)]
    for quarter in range(NY):
        cols = slice(quarter * 512, quarter * 512 + 512)
        result = acc_out[:, cols]
        for side in range(2):
            result = result + jnp.dot(
                sides[side], w_buf[quarter, side, 1], preferred_element_type=F32
            )
        out_ref[:, cols] = result.astype(BF16)

    for condition, count in ((local, 7), (jnp.logical_not(local), 8)):

        @pl.when(condition)
        def _(count=count):
            ref = lsend.at[pl.ds(0, count)]
            remote(ref, ref, log_ss, log_rs, partner).wait()

    for head in range(4):
        for half in range(2):
            for which_map in range(2):
                log_ref[which_map, head : head + 1, half * HALF : half * HALF + HALF] = log_buf[
                    head, half, which_map : which_map + 1, :
                ]

    for kind in range(3):
        for condition, count in ((local, 7), (jnp.logical_not(local), 8)):

            @pl.when(condition)
            def _(kind=kind, count=count):
                ref = k_buf.at[0, pl.ds(0, HALF * count), :]
                remote(ref, ref, z_ss.at[kind], z_rs.at[0, 0], partner).wait_send()

    for copy in pending:
        copy.wait_send()
    sent_all(0)
    sent_all(1)
    ref = ret_send.at[pl.ds(0, NZ - 1)]
    remote(ref, ref, ret_ss, ret_rs, partner).wait_send()
    ref = w_buf.at[:, :, :, pl.ds(0, 448), :]
    remote(ref, ref, w_ss, w_rs.at[0, 0], partner).wait_send()


def hand_over(mixed_ref, logs_ref, mixed_out, logs_out):
    mixed_out[...] = mixed_ref[...]
    logs_out[...] = logs_ref[...]


def body(
    inputs,
    norm_gain,
    w_glu_value,
    w_glu_gate,
    w_query_one,
    w_query_two,
    w_key_one,
    w_key_two,
    w_value,
    conv_kernel,
    conv_gain,
    head_gain,
    lambda_head,
    w_out_conv,
    w_out_attn,
):
    vmem = pl.BlockSpec(memory_space=pltpu.VMEM)
    hbm = pl.BlockSpec(memory_space=pl.ANY)
    dma = pltpu.SemaphoreType.DMA
    mixed, logs = pl.pallas_call(
        kernel,
        out_shape=(
            jax.ShapeDtypeStruct((HALF, D), BF16),
            jax.ShapeDtypeStruct((2, 4, 2 * HALF), F32),
        ),
        in_specs=[vmem] * 5 + [pl.BlockSpec(memory_space=pltpu.SMEM)] + [hbm] * 9,
        out_specs=(vmem, vmem),
        scratch_shapes=[
            pltpu.VMEM((D, 512), BF16),
            pltpu.VMEM((D, 512), BF16),
            pltpu.VMEM((D, 256), BF16),
            pltpu.VMEM((D, 256), BF16),
            pltpu.VMEM((D, 256), BF16),
            pltpu.VMEM((D, 256), BF16),
            pltpu.VMEM((D, 512), BF16),
            pltpu.VMEM((2 * HALF, D), BF16),
            pltpu.VMEM((4, 2, HALF, 128), BF16),
            pltpu.VMEM((4, 2, HALF, 128), BF16),
            pltpu.VMEM((4, 2, HALF, 128), BF16),
            pltpu.VMEM((NZ, NX * 2 * HALF, 128), BF16),
            pltpu.VMEM((NZ, NX * 2 * HALF, 128), BF16),
            pltpu.VMEM((NZ, HALF, 128), BF16),
            pltpu.VMEM((NZ, 2 * HALF, 128), BF16),
            pltpu.VMEM((2 * HALF + 32, 512), F32),
            pltpu.VMEM((32, 512), BF16),
            pltpu.VMEM((32, 512), BF16),
            pltpu.VMEM((2 * HALF, 512), F32),
            pltpu.VMEM((2 * HALF, 128), F32),
            pltpu.VMEM((2 * HALF, 128), F32),
            pltpu.VMEM((2, HALF, 512), BF16),
            pltpu.VMEM((HALF, 512), BF16),
            pltpu.VMEM((NZ, 8, 256), F32),
            pltpu.VMEM((NZ, 144, 256), F32),
            pltpu.VMEM((1024, 256), F32),
            pltpu.VMEM((1024, 256), F32),
            pltpu.VMEM((8, 256), F32),
            pltpu.VMEM((8, 256), F32),
            pltpu.VMEM((2, 16, 8, 256), F32),
            pltpu.VMEM((128, 128), F32),
            pltpu.VMEM((NZ, HALF, 128), BF16),
            pltpu.VMEM((NZ, HALF, 128), BF16),
            pltpu.VMEM((NZ, 8, 128), F32),
            pltpu.VMEM((4, 2, 8, 128), F32),
            pltpu.VMEM((8, 128), F32),
            pltpu.VMEM((8, 128), F32),
            pltpu.VMEM((NY, 2, 2, 512, 512), BF16),
            pltpu.VMEM((HALF, D), F32),
            dma((7,)),
            dma((2,)),
            dma((3,)),
            dma((3, NZ)),
            dma((2,)),
            dma((2, 2, NZ)),
            dma((2,)),
            dma((2, NZ)),
            dma((2,)),
            dma((2,)),
            dma((2,)),
            dma((2,)),
            dma,
            dma,
            dma,
            dma,
            dma,
            dma((3, 2)),
            dma((3, 2)),
            dma((2,)),
            dma((2,)),
        ],
        compiler_params=pltpu.CompilerParams(
            collective_id=0, has_side_effects=True, vmem_limit_bytes=60 * 1024 * 1024
        ),
        name="mixer",
    )(
        inputs[0],
        norm_gain[None],
        conv_kernel,
        conv_gain[None],
        head_gain[None],
        lambda_head,
        w_glu_value,
        w_glu_gate,
        w_query_one,
        w_query_two,
        w_key_one,
        w_key_two,
        w_value,
        w_out_conv,
        w_out_attn,
    )
    mixed, logs = pl.pallas_call(
        hand_over,
        out_shape=(
            jax.ShapeDtypeStruct((HALF, D), BF16),
            jax.ShapeDtypeStruct((2, 4, 2 * HALF), F32),
        ),
        in_specs=[vmem, vmem],
        out_specs=(vmem, vmem),
        name="hand_over",
    )(mixed, logs)
    return (mixed[None], logs[None])


def solution(mesh):
    return jax.shard_map(
        body,
        mesh=mesh,
        in_specs=(
            P("fs", ("sp", "tp"), None),
            P(),
            P(None, "tp"),
            P(None, "tp"),
            P(None, "tp"),
            P(None, "tp"),
            P(None, "tp"),
            P(None, "tp"),
            P(None, "tp"),
            P(None, "tp"),
            P("tp"),
            P(),
            P("tp"),
            P("tp", "fs"),
            P("tp", "fs"),
        ),
        out_specs=(P("fs", ("sp", "tp"), None), P("fs", None, "tp", "sp")),
        check_vma=False,
    )
```

```python
import jax
import jax.numpy as jnp
from jax import lax
from jax.experimental import pallas as pl
from jax.experimental.pallas import tpu as pltpu
from jax.sharding import PartitionSpec as P

D = 2048
DC = 1024
HD = 64
CW = 31
NZ = 8
NX = 4
NY = 4
HALF = 128
Z_GATE = 0
Q_GATE = 4
FAR_FIRST = (0, 4, 5, 3, 6, 2, 7, 1)
V_SPLIT = 4
W_THREE = 5
NEG_FILL = -1e30
EPSILON = 1e-05
HEAD_SCALE = 0.8
MESH = pl.DeviceIdType.MESH
F32 = jnp.float32
BF16 = jnp.bfloat16


def remote(src, dst, send_sem, recv_sem, device):
    return pltpu.make_async_remote_copy(
        src_ref=src,
        dst_ref=dst,
        send_sem=send_sem,
        recv_sem=recv_sem,
        device_id=device,
        device_id_type=MESH,
    )


def kernel(
    x_ref,
    gain_ref,
    ck_ref,
    cg_ref,
    hg_ref,
    lam_ref,
    wgv_hbm,
    wgg_hbm,
    wq1_hbm,
    wq2_hbm,
    wk1_hbm,
    wk2_hbm,
    wv_hbm,
    woc_hbm,
    woa_hbm,
    out_ref,
    log_ref,
    wgv,
    wgg,
    wq1,
    wq2,
    wk1,
    wk2,
    wv,
    normed,
    k_send,
    v_send,
    q_send,
    k_buf,
    v_buf,
    q_raw,
    qs,
    gated_ext,
    halo_send,
    halo_recv,
    convd,
    sums_send,
    sums_recv,
    conv_full,
    conv_send,
    m_buf,
    acc,
    score_a,
    score_b,
    max_a,
    max_b,
    bias,
    gain_t,
    ret_send,
    attn_buf,
    lsend,
    log_buf,
    lam_own,
    lam_recv,
    w_buf,
    acc_out,
    load_sem,
    norm_sem,
    z_ss,
    z_rs,
    xs_ss,
    xs_rs,
    d_ss,
    d_rs,
    halo_sem,
    sums_sem,
    cx_sem,
    lam_sem,
    ret_ss,
    ret_rs,
    log_ss,
    log_rs,
    w_ss,
    w_rs,
    wx_rs,
    wd_rs,
    own_sem,
):
    me = lax.axis_index("sp")
    y = lax.axis_index("fs")
    c = lax.axis_index("tp")
    z, x = me // NX, me % NX
    other = 1 - c
    xr, xl, xo = (x + 1) % NX, (x + 3) % NX, (x + 2) % NX
    yr, yl, yo = (y + 1) % NY, (y + 3) % NY, (y + 2) % NY
    src_tp = z // 4
    own_head = z % 4
    local = src_tp == c
    partner = {"tp": other}
    right = {"sp": z * NX + xr}
    left = {"sp": z * NX + xl}
    up = {"fs": yr}
    down = {"fs": yl}
    following = {"sp": (me + 1) % (NZ * NX)}
    preceding = {"sp": (me + NZ * NX - 1) % (NZ * NX)}
    pending = []

    def begin(copy):
        copy.start()
        pending.append(copy)
        return copy

    loads = []
    for index, (src, dst) in enumerate(
        ((wk1_hbm, wk1), (wk2_hbm, wk2), (wv_hbm, wv), (wq1_hbm, wq1), (wq2_hbm, wq2),
         (wgv_hbm, wgv), (wgg_hbm, wgg))
    ):
        loads.append(pltpu.make_async_copy(src, dst, load_sem.at[index]))
        if index < 2:
            loads[-1].start()

    barrier = pltpu.get_barrier_semaphore()
    for device in (partner, right, left, up, down, following, preceding):
        pl.semaphore_signal(barrier, inc=1, device_id=device, device_id_type=MESH)
    for step in range(1, NZ):
        for core in range(2):
            pl.semaphore_signal(
                barrier,
                inc=1,
                device_id={"sp": ((z + step) % NZ) * NX + x, "tp": core},
                device_id_type=MESH,
            )

    my_rows = pl.multiple_of(c * HALF, HALF)
    peer_rows = pl.multiple_of(other * HALF, HALF)
    for part in range(4):
        rows_f = x_ref[part * 32 : part * 32 + 32, :].astype(F32)
        scale = lax.rsqrt(jnp.mean(rows_f * rows_f, axis=-1, keepdims=True) + EPSILON)
        normed[pl.ds(my_rows + part * 32, 32), :] = (rows_f * scale * gain_ref[...]).astype(BF16)

    lane = lax.broadcasted_iota(jnp.int32, (HALF, 128), 1)
    low = lane < HD

    def head_pair(one, two, head):
        pair = slice((head // 2) * 128, (head // 2) * 128 + 128)
        first, second = one[:, pair], two[:, pair]
        if head % 2 == 0:
            return jnp.where(low, first, pltpu.roll(second, HD, 1))
        return jnp.where(low, pltpu.roll(first, HD, 1), second)

    def project(rows, index, weight, fresh):
        if fresh:
            loads[index].wait()
        return jnp.dot(normed[pl.ds(rows, HALF), :], weight[...], preferred_element_type=F32)

    def project_keys(rows, half, fresh):
        one = project(rows, 0, wk1, fresh)
        two = project(rows, 1, wk2, fresh)
        for head in range(4):
            k_send[head, half] = head_pair(one, two, head).astype(BF16)

    def project_values(rows, half, fresh):
        values = project(rows, 2, wv, fresh)
        for head in range(4):
            v_send[head, half] = jnp.transpose(values[:, head * 128 : head * 128 + 128]).astype(BF16)

    def project_queries(rows, half, fresh):
        one = project(rows, 3, wq1, fresh)
        two = project(rows, 4, wq2, fresh)
        for head in range(4):
            q_send[head, half] = (head_pair(one, two, head) * (HD**-0.5)).astype(BF16)

    def project_glu(rows, fresh):
        block = normed[pl.ds(rows, HALF), :]
        if fresh:
            loads[5].wait()
            loads[6].wait()
        value = jnp.dot(block, wgv[...], preferred_element_type=F32).astype(BF16).astype(F32)
        gate = jnp.dot(block, wgg[...], preferred_element_type=F32).astype(BF16).astype(F32)
        gated = (value * jax.nn.sigmoid(gate)).astype(BF16)
        gated_ext[pl.ds(pl.multiple_of(rows + 32, 32), HALF), :] = gated.astype(F32)

    project_keys(my_rows, c, True)
    for load in loads[2:]:
        load.start()
    for index in range(4):
        lam_own[index : index + 1, :] = jnp.full((1, 128), lam_ref[index], F32)
    lam_own[4:8, :] = jnp.zeros((4, 128), F32)

    pl.semaphore_wait(barrier, 7 + 2 * (NZ - 1))

    mine = normed.at[pl.ds(my_rows, HALF), :]
    norm_copy = begin(remote(mine, mine, norm_sem.at[0], norm_sem.at[1], partner))

    blocks = (k_buf, v_buf)

    def slot(kind, zs, xs, cs):
        return blocks[kind].at[zs, pl.ds(pl.multiple_of((xs * 2 + cs) * HALF, HALF), HALF), :]

    def slot_half(kind, zs, xs, cs, part):
        start = pl.multiple_of((xs * 2 + cs) * HALF + part * (HALF // 2), HALF // 2)
        return blocks[kind].at[zs, pl.ds(start, HALF // 2), :]

    u = z % 4
    ranks = (u, u + 1 - 2 * (u % 2), 2 - u // 2, 3 * (1 - u // 2))
    same = 1 - src_tp - c + 2 * src_tp * c

    sources = (k_send, v_send, q_send)

    def z_send(kind, half):
        for rank in (3, 2, 1, 0):
            head = same * ranks[rank] + (1 - same) * ranks[3 - rank]
            target = 4 * c + head
            landing = q_raw.at[z] if kind == 2 else slot(kind, z, x, half)
            copy = remote(
                sources[kind].at[head, half],
                landing,
                z_ss.at[kind],
                z_rs.at[kind, z],
                {"sp": target * NX + x, "tp": half},
            )
            away = jnp.logical_not((target == z) & (half == c))

            @pl.when(away)
            def _(copy=copy):
                copy.start()

    z_send(0, c)
    project_values(my_rows, c, True)

    @pl.when(local)
    def _():
        mine = pl.ds(pl.multiple_of((x * 2 + c) * HALF, HALF), HALF)
        k_buf[z, mine, :] = k_send[own_head, c]
        v_buf[z, mine, :] = v_send[own_head, c]

    def z_wait(kind, zs):
        ref = q_raw.at[zs] if kind == 2 else slot(kind, zs, x, c)

        @pl.when(jnp.logical_not((zs == z) & local))
        def _():
            remote(ref, ref, z_ss.at[kind], z_rs.at[kind, zs], partner).wait_recv()

    def pass_on(kind, ref, arrival, device):
        remote(ref, ref, xs_ss.at[kind], arrival, device).start()

    def share(kind, ref, zs):
        remote(ref, ref, d_ss.at[kind], d_rs.at[kind, zs], partner).start()

    def arrive(kind, rows, arrival):
        ref = blocks[kind].at[0, pl.ds(0, rows), :]
        remote(ref, ref, xs_ss.at[kind], arrival, partner).wait_recv()

    def stage_one(kind, zs):
        ref = slot(kind, zs, x, c)
        pass_on(kind, ref, xs_rs.at[kind, 0, zs], right)
        pass_on(kind, ref, xs_rs.at[kind, 0, zs], left)
        share(kind, ref, zs)

    w_hbm = (woc_hbm, woa_hbm)

    def w_own(side, kind, device):
        remote(w_hbm[kind], w_buf.at[y, c, kind], w_ss, w_rs.at[side, kind], device).start()

    w_own(0, 0, up)
    w_own(1, 1, down)
    lam_copy = begin(remote(lam_own, lam_recv, lam_sem.at[0], lam_sem.at[1], partner))

    project_glu(my_rows, True)
    norm_copy.wait_recv()
    project_keys(peer_rows, other, False)
    z_send(0, other)
    project_glu(peer_rows, False)
    halo_send[...] = gated_ext[2 * HALF :, :].astype(BF16)
    halo_copy = begin(remote(halo_send, halo_recv, halo_sem.at[0], halo_sem.at[1], following))
    project_values(peer_rows, other, False)
    z_wait(0, z)
    stage_one(0, z)
    project_queries(my_rows, c, True)
    project_queries(peer_rows, other, False)

    @pl.when(local)
    def _():
        q_raw[z] = q_send[own_head, c]

    own_w = []
    for kind in range(2):
        own = pltpu.make_async_copy(w_hbm[kind], w_buf.at[y, c, kind], own_sem.at[kind])
        own.start()
        own_w.append(own)
        remote(w_hbm[kind], w_buf.at[y, c, kind], w_ss, wd_rs.at[kind], partner).start()

    taps = ck_ref[...].astype(F32)

    def conv_chunk(part):
        base = part * 32
        total = None
        for shift in range(8):
            partial = None
            span = 32 if shift == 0 else 40
            for group in range(5):
                tap = 8 * group + shift - 2
                if tap < 0 or tap >= CW:
                    continue
                term = taps[tap : tap + 1, :] * gated_ext[base + 8 * group : base + 8 * group + span, :]
                partial = term if partial is None else partial + term
            moved = partial[shift : shift + 32, :]
            total = moved if total is None else total + moved
        convd[base : base + 32, :] = total
        sums = jnp.sum(total, axis=-1, keepdims=True)
        squares = jnp.sum(total * total, axis=-1, keepdims=True)
        sums_send[base : base + 32, :] = jnp.where(low[:32], sums, squares)

    def stage_queries(zs):
        z_wait(2, zs)
        rows = q_raw[zs]
        zero = jnp.zeros_like(rows)
        qs[zs, :HALF] = jnp.where(low, rows, zero)
        qs[zs, HALF:] = jnp.where(low, zero, rows)

    def stage_two(kind, zs):
        arrive(kind, 2 * HALF, xs_rs.at[kind, 0, zs])
        pass_on(kind, slot_half(kind, zs, xl, c, 0), xs_rs.at[kind, 1, zs], right)
        pass_on(kind, slot_half(kind, zs, xr, c, 1), xs_rs.at[kind, 1, zs], left)
        share(kind, slot(kind, zs, xl, c), zs)
        share(kind, slot(kind, zs, xr, c), zs)

    def stage_three(kind, zs):
        arrive(kind, HALF, xs_rs.at[kind, 1, zs])
        share(kind, slot(kind, zs, xo, c), zs)

    def stage_four(kind, zs):
        arrive(kind, 4 * HALF, d_rs.at[kind, zs])

    def sent_all(kind):
        ref = blocks[kind].at[pl.ds(0, 3)]
        remote(ref, ref, xs_ss.at[kind], d_rs.at[0, 0], partner).wait_send()
        ref = blocks[kind].at[pl.ds(0, 4)]
        remote(ref, ref, d_ss.at[kind], d_rs.at[0, 0], partner).wait_send()

    def w_wait(ref, arrival):
        remote(ref, ref, w_ss, arrival, partner).wait_recv()

    def w_pass(ref, arrival, device):
        remote(ref, ref, w_ss, arrival, device).start()

    def piece(source, core, kind, xs):
        return w_buf.at[source, core, kind, pl.ds(pl.multiple_of(xs * 128, 128), 128), :]

    def w_one():
        w_wait(w_buf.at[yl, c, 0], w_rs.at[0, 0])
        w_pass(piece(yl, c, 0, x), w_rs.at[2, 0], up)
        w_own(0, 1, up)
        w_wait(w_buf.at[yr, c, 1], w_rs.at[1, 1])
        w_pass(piece(yr, c, 1, x), w_rs.at[2, 1], down)
        w_own(1, 0, down)
        w_pass(w_buf.at[yl, c, 0], wd_rs.at[0], partner)
        w_pass(w_buf.at[yr, c, 1], wd_rs.at[1], partner)

    def w_two():
        for kind in range(2):
            ref = piece(yo, c, kind, x)
            w_wait(ref, w_rs.at[2, kind])
            w_pass(ref, wx_rs.at[0, kind], right)
            w_pass(ref, wx_rs.at[1, kind], left)
            w_pass(ref, wd_rs.at[kind], partner)

    def w_three():
        for kind in range(2):
            for side, xs in ((0, xl), (1, xr)):
                ref = piece(yo, c, kind, xs)
                w_wait(ref, wx_rs.at[side, kind])
                if side == kind:
                    w_pass(ref, wx_rs.at[2, kind], right if side == 0 else left)
                w_pass(ref, wd_rs.at[kind], partner)

    def w_four():
        w_wait(w_buf.at[yr, c, 0], w_rs.at[1, 0])
        w_pass(w_buf.at[yr, c, 0], wd_rs.at[0], partner)
        w_wait(piece(yo, c, 0, xo), wx_rs.at[2, 0])
        w_pass(piece(yo, c, 0, xo), wd_rs.at[0], partner)
        w_wait(w_buf.at[yl, c, 1], w_rs.at[0, 1])
        w_pass(w_buf.at[yl, c, 1], wd_rs.at[1], partner)
        w_wait(piece(yo, c, 1, xo), wx_rs.at[2, 1])
        w_pass(piece(yo, c, 1, xo), wd_rs.at[1], partner)

    def w_five(kind):
        w_wait(w_buf.at[0], wd_rs.at[kind])

    def conv_finish():
        sums_copy.wait_recv()
        for half in range(2):
            rows = slice(half * HALF, half * HALF + HALF)
            row_sums = sums_send[rows, :] + sums_recv[rows, :]
            mean = row_sums[:, 0:1] * (1.0 / DC)
            square = row_sums[:, HD : HD + 1] * (1.0 / DC)
            scaled = (convd[rows, :] - mean) * lax.rsqrt(square - mean * mean + EPSILON) * cg_ref[...]
            result = (scaled * jax.nn.sigmoid(scaled)).astype(BF16)

            @pl.when(c == half)
            def _(result=result):
                conv_full[c] = result

            @pl.when(c != half)
            def _(result=result):
                conv_send[...] = result

        return begin(remote(conv_send, conv_full.at[c], cx_sem.at[0], cx_sem.at[1], partner))

    m_buf[...] = jnp.full_like(m_buf, NEG_FILL)
    acc[...] = jnp.zeros_like(acc)
    bias[0] = jnp.zeros((16, 8, 256), F32)
    query_segment = (x * 4 + c * 2) + (
        (lax.broadcasted_iota(jnp.int32, (8, 256), 1) & (HALF - 1)) >> 6
    )
    for segment in range(16):
        bias[1, segment] = jnp.where(query_segment >= segment, 0.0, NEG_FILL)
    gain_t[...] = jnp.transpose(jnp.broadcast_to(hg_ref[...], (128, 128))) * HEAD_SCALE

    def place(index):
        return (z + FAR_FIRST[index]) % NZ

    before = (z * (z + 1)) // 2

    def which(t):
        skipped = t + jnp.where(t >= before, z + 1, 0)
        t = jnp.where(t >= 35 - z, t - 35 + z + before, skipped)
        i = 0
        for bound in (1, 3, 6, 10, 15, 21, 28):
            i = i + jnp.where(t >= bound, 1, 0)
        j = t - (i * (i + 1)) // 2
        return j, i, (j + 1) // (i + 1)

    def scores(t, score_ref, max_ref):
        s, zt, kind = which(t)
        queries = qs[zt]
        best = None
        for start in range(0, 1024, 256):
            block = lax.dot_general(
                k_buf[s, start : start + 256, :],
                queries,
                (((1,), (1,)), ((), ())),
                preferred_element_type=F32,
            )
            score_ref[start : start + 256] = block
            for inner in range(4):
                top = None
                for row in range(inner * 64, inner * 64 + 64, 8):
                    top = block[row : row + 8] if top is None else jnp.maximum(top, block[row : row + 8])
                top = top + bias[kind, start // 64 + inner]
                best = top if best is None else jnp.maximum(best, top)
        max_ref[...] = best

    ones = jnp.ones((16, 256), BF16)

    def absorb(t, score_ref, max_ref):
        s, zt, kind = which(t)
        old = m_buf[zt, 0:1]
        new = jnp.maximum(old, jnp.max(max_ref[...], axis=0, keepdims=True))
        factor = jnp.exp(old - new)
        total = None
        for start in range(0, 1024, 256):
            weights = []
            for inner in range(4):
                row = start + inner * 64
                shifted = new - bias[kind, row // 64, 0:1]
                weights.append(jnp.exp(score_ref[row : row + 64] - shifted).astype(BF16))
            lhs = jnp.concatenate(
                [
                    jnp.concatenate(
                        [
                            v_buf[s, start : start + 128, :],
                            v_buf[s, start + 128 : start + 256, :],
                        ],
                        axis=1,
                    ),
                    ones,
                ],
                axis=0,
            )
            part = jnp.dot(lhs, jnp.concatenate(weights, axis=0), preferred_element_type=F32)
            total = part if total is None else total + part
        acc[zt] = acc[zt] * factor + total
        m_buf[zt] = jnp.broadcast_to(new, (8, 256))

    def ret_copy(s):
        return remote(
            ret_send.at[s], attn_buf.at[z], ret_ss, ret_rs, {"sp": s * NX + x}
        )

    def log_copy(s):
        return remote(
            lsend.at[s], log_buf.at[own_head, c], log_ss, log_rs,
            {"sp": s * NX + x, "tp": src_tp},
        )

    def finish(s):
        sums = acc[s, 128:129, :]
        normal = acc[s, 0:128, :] * (1.0 / sums)
        lam_row = jnp.where(local, lam_own[pl.ds(own_head, 1), :], lam_recv[pl.ds(own_head, 1), :])
        head_out = normal[:, :HALF] - lam_row * normal[:, HALF:]
        head_out = (
            head_out
            * lax.rsqrt(jnp.mean(head_out * head_out, axis=0, keepdims=True) + EPSILON)
            * gain_t[...]
        )
        head_out = jnp.transpose(head_out).astype(BF16)
        logs = m_buf[s, 0:1] + jnp.log(sums)
        sub = lax.broadcasted_iota(jnp.int32, (8, 128), 0)
        log_rows = jnp.where(sub == 0, logs[:, :HALF], logs[:, HALF:])
        ret_send[s] = head_out
        lsend[s] = log_rows

        @pl.when(s == z)
        def _():
            attn_buf[z] = head_out

        @pl.when((s == z) & local)
        def _():
            log_buf[own_head, c] = log_rows

        @pl.when(s != z)
        def _():
            ret_copy(s).start()

        @pl.when(jnp.logical_not((s == z) & local))
        def _():
            log_copy(s).start()

    def finish_one_of(t):
        _, first, first_done = which(t)
        _, second, second_done = which(t + 1)

        def run(_, carry):
            finish(first * first_done + second * second_done)
            return carry

        lax.fori_loop(0, first_done + second_done, run, 0)

    def pair(p, carry):
        scores(2 * p + 1, score_b, max_b)
        absorb(2 * p, score_a, max_a)
        scores(2 * p + 2, score_a, max_a)
        absorb(2 * p + 1, score_b, max_b)
        finish_one_of(2 * p)
        return carry

    for step in range(NZ):
        if step > 0:
            z_wait(0, place(step))
            stage_one(0, place(step))
        if step == Z_GATE:
            z_send(1, c)
            z_send(1, other)
    for step in range(NZ):
        stage_two(0, place(step))
        if step > 0:
            conv_chunk(step)
        if step == Q_GATE:
            z_send(2, c)
            z_send(2, other)
    for step in range(NZ):
        z_wait(1, place(step))
    for step in range(V_SPLIT):
        stage_one(1, step)
    w_one()
    for step in range(NZ):
        stage_three(0, place(step))
    halo_copy.wait_recv()
    rows = halo_recv[...].astype(F32)
    gated_ext[0:32, :] = jnp.where(me == 0, jnp.zeros_like(rows), rows)
    conv_chunk(0)
    sums_copy = begin(remote(sums_send, sums_recv, sums_sem.at[0], sums_sem.at[1], partner))
    for step in range(V_SPLIT):
        stage_two(1, step)
    for step in range(V_SPLIT, NZ):
        stage_one(1, step)
    conv_copy = conv_finish()
    for step in range(V_SPLIT):
        stage_three(1, step)
    lam_copy.wait_recv()
    for step in range(NZ):
        stage_four(0, place(step))
    stage_queries(0)
    stage_four(1, 0)
    done_pairs = 0
    for index in range(NZ):
        if index + 1 < NZ:
            stage_queries(index + 1)
            stage_four(1, index + 1)
        if index == 0:
            scores(0, score_a, max_a)
        else:
            end = ((index + 1) * (index + 2) // 2 - 1) // 2
            lax.fori_loop(done_pairs, end, pair, 0)
            done_pairs = end
        if index == 0:
            for step in range(V_SPLIT, NZ):
                stage_two(1, step)
        if index == V_SPLIT - 2:
            for step in range(V_SPLIT, NZ):
                stage_three(1, step)
            w_two()
        if index == W_THREE:
            w_three()
    w_four()
    scores(35, score_b, max_b)
    absorb(34, score_a, max_a)
    absorb(35, score_b, max_b)

    def run_last(_, carry):
        finish(NZ - 1)
        return carry

    lax.fori_loop(0, (7 - z) // 7, run_last, 0)

    finish(z)

    for kind in range(2):
        own_w[kind].wait()
    conv_copy.wait_recv()
    w_five(0)
    for quarter in range(NY):
        cols = slice(quarter * 512, quarter * 512 + 512)
        acc_out[:, cols] = jnp.dot(
            conv_full[0], w_buf[quarter, 0, 0], preferred_element_type=F32
        ) + jnp.dot(conv_full[1], w_buf[quarter, 1, 0], preferred_element_type=F32)
    w_five(1)

    ref = ret_send.at[pl.ds(0, NZ - 1)]
    remote(ref, ref, ret_ss, ret_rs, partner).wait_recv()

    sides = [jnp.concatenate([attn_buf[4 * side + k] for k in range(4)], axis=1) for side in range(2)]
    for quarter in range(NY):
        cols = slice(quarter * 512, quarter * 512 + 512)
        result = acc_out[:, cols]
        for side in range(2):
            result = result + jnp.dot(
                sides[side], w_buf[quarter, side, 1], preferred_element_type=F32
            )
        out_ref[:, cols] = result.astype(BF16)

    for condition, count in ((local, 7), (jnp.logical_not(local), 8)):

        @pl.when(condition)
        def _(count=count):
            ref = lsend.at[pl.ds(0, count)]
            remote(ref, ref, log_ss, log_rs, partner).wait()

    for head in range(4):
        for half in range(2):
            for which_map in range(2):
                log_ref[which_map, head : head + 1, half * HALF : half * HALF + HALF] = log_buf[
                    head, half, which_map : which_map + 1, :
                ]

    for kind in range(3):
        for condition, count in ((local, 7), (jnp.logical_not(local), 8)):

            @pl.when(condition)
            def _(kind=kind, count=count):
                ref = k_buf.at[0, pl.ds(0, HALF * count), :]
                remote(ref, ref, z_ss.at[kind], z_rs.at[0, 0], partner).wait_send()

    for copy in pending:
        copy.wait_send()
    sent_all(0)
    sent_all(1)
    ref = ret_send.at[pl.ds(0, NZ - 1)]
    remote(ref, ref, ret_ss, ret_rs, partner).wait_send()
    ref = w_buf.at[:, :, :, pl.ds(0, 448), :]
    remote(ref, ref, w_ss, w_rs.at[0, 0], partner).wait_send()


def hand_over(mixed_ref, logs_ref, mixed_out, logs_out):
    mixed_out[...] = mixed_ref[...]
    logs_out[...] = logs_ref[...]


def body(
    inputs,
    norm_gain,
    w_glu_value,
    w_glu_gate,
    w_query_one,
    w_query_two,
    w_key_one,
    w_key_two,
    w_value,
    conv_kernel,
    conv_gain,
    head_gain,
    lambda_head,
    w_out_conv,
    w_out_attn,
):
    vmem = pl.BlockSpec(memory_space=pltpu.VMEM)
    hbm = pl.BlockSpec(memory_space=pl.ANY)
    dma = pltpu.SemaphoreType.DMA
    mixed, logs = pl.pallas_call(
        kernel,
        out_shape=(
            jax.ShapeDtypeStruct((HALF, D), BF16),
            jax.ShapeDtypeStruct((2, 4, 2 * HALF), F32),
        ),
        in_specs=[vmem] * 5 + [pl.BlockSpec(memory_space=pltpu.SMEM)] + [hbm] * 9,
        out_specs=(vmem, vmem),
        scratch_shapes=[
            pltpu.VMEM((D, 512), BF16),
            pltpu.VMEM((D, 512), BF16),
            pltpu.VMEM((D, 256), BF16),
            pltpu.VMEM((D, 256), BF16),
            pltpu.VMEM((D, 256), BF16),
            pltpu.VMEM((D, 256), BF16),
            pltpu.VMEM((D, 512), BF16),
            pltpu.VMEM((2 * HALF, D), BF16),
            pltpu.VMEM((4, 2, HALF, 128), BF16),
            pltpu.VMEM((4, 2, HALF, 128), BF16),
            pltpu.VMEM((4, 2, HALF, 128), BF16),
            pltpu.VMEM((NZ, NX * 2 * HALF, 128), BF16),
            pltpu.VMEM((NZ, NX * 2 * HALF, 128), BF16),
            pltpu.VMEM((NZ, HALF, 128), BF16),
            pltpu.VMEM((NZ, 2 * HALF, 128), BF16),
            pltpu.VMEM((2 * HALF + 32, 512), F32),
            pltpu.VMEM((32, 512), BF16),
            pltpu.VMEM((32, 512), BF16),
            pltpu.VMEM((2 * HALF, 512), F32),
            pltpu.VMEM((2 * HALF, 128), F32),
            pltpu.VMEM((2 * HALF, 128), F32),
            pltpu.VMEM((2, HALF, 512), BF16),
            pltpu.VMEM((HALF, 512), BF16),
            pltpu.VMEM((NZ, 8, 256), F32),
            pltpu.VMEM((NZ, 144, 256), F32),
            pltpu.VMEM((1024, 256), F32),
            pltpu.VMEM((1024, 256), F32),
            pltpu.VMEM((8, 256), F32),
            pltpu.VMEM((8, 256), F32),
            pltpu.VMEM((2, 16, 8, 256), F32),
            pltpu.VMEM((128, 128), F32),
            pltpu.VMEM((NZ, HALF, 128), BF16),
            pltpu.VMEM((NZ, HALF, 128), BF16),
            pltpu.VMEM((NZ, 8, 128), F32),
            pltpu.VMEM((4, 2, 8, 128), F32),
            pltpu.VMEM((8, 128), F32),
            pltpu.VMEM((8, 128), F32),
            pltpu.VMEM((NY, 2, 2, 512, 512), BF16),
            pltpu.VMEM((HALF, D), F32),
            dma((7,)),
            dma((2,)),
            dma((3,)),
            dma((3, NZ)),
            dma((2,)),
            dma((2, 2, NZ)),
            dma((2,)),
            dma((2, NZ)),
            dma((2,)),
            dma((2,)),
            dma((2,)),
            dma((2,)),
            dma,
            dma,
            dma,
            dma,
            dma,
            dma((3, 2)),
            dma((3, 2)),
            dma((2,)),
            dma((2,)),
        ],
        compiler_params=pltpu.CompilerParams(
            collective_id=0, has_side_effects=True, vmem_limit_bytes=60 * 1024 * 1024
        ),
        name="mixer",
    )(
        inputs[0],
        norm_gain[None],
        conv_kernel,
        conv_gain[None],
        head_gain[None],
        lambda_head,
        w_glu_value,
        w_glu_gate,
        w_query_one,
        w_query_two,
        w_key_one,
        w_key_two,
        w_value,
        w_out_conv,
        w_out_attn,
    )
    mixed, logs = pl.pallas_call(
        hand_over,
        out_shape=(
            jax.ShapeDtypeStruct((HALF, D), BF16),
            jax.ShapeDtypeStruct((2, 4, 2 * HALF), F32),
        ),
        in_specs=[vmem, vmem],
        out_specs=(vmem, vmem),
        name="hand_over",
    )(mixed, logs)
    return (mixed[None], logs[None])


def solution(mesh):
    return jax.shard_map(
        body,
        mesh=mesh,
        in_specs=(
            P("fs", ("sp", "tp"), None),
            P(),
            P(None, "tp"),
            P(None, "tp"),
            P(None, "tp"),
            P(None, "tp"),
            P(None, "tp"),
            P(None, "tp"),
            P(None, "tp"),
            P(None, "tp"),
            P("tp"),
            P(),
            P("tp"),
            P("tp", "fs"),
            P("tp", "fs"),
        ),
        out_specs=(P("fs", ("sp", "tp"), None), P("fs", None, "tp", "sp")),
        check_vma=False,
    )
```
